32 devices in a mesh: ep: 4 (over y, x), tp: 8 (over z, core).
Axes of the slice: x: 2, y: 2, z: 4, core: 2. Of those that a mesh axis runs over, the one named last changes fastest.
Arguments:
- resid: bfloat16 [512, 2048], P('ep'), may hold values from -6 to 6
- norm1_gain: float32 [2048], replicated, may hold values from 0.1 to 1.9
- w_query: bfloat16 [2048, 2048], P('ep', 'tp'), may hold values from -0.125 to 0.125
- w_key: bfloat16 [2048, 2048], P('ep', 'tp'), may hold values from -0.125 to 0.125
- w_value: bfloat16 [2048, 2048], P('ep', 'tp'), may hold values from -0.125 to 0.125
- w_outgate: bfloat16 [2048, 2048], P('ep', 'tp'), may hold values from -0.125 to 0.125
- w_igate: bfloat16 [2048, 32], replicated, may hold values from -0.125 to 0.125
- w_fgate: bfloat16 [2048, 32], replicated, may hold values from -0.125 to 0.125
- forget_bias: float32 [32], replicated, may hold values from 0 to 4
- head_gain: float32 [2048], P('tp'), may hold values from 0.1 to 1.9
- w_out: bfloat16 [2048, 2048], P('tp'), may hold values from -0.125 to 0.125
- state_matrix: float32 [512, 32, 64, 64], P('ep', 'tp'), may hold values from -4 to 4
- state_norm: float32 [512, 32, 64], P('ep', 'tp'), may hold values from -8 to 8
- state_max: float32 [512, 32], P('ep', 'tp'), may hold values from -1 to 2
- norm2_gain: float32 [2048], replicated, may hold values from 0.1 to 1.9
- group_router: bfloat16 [2048, 4], replicated, may hold values from -0.125 to 0.125
- expert_router: bfloat16 [2048, 8], replicated, may hold values from -0.125 to 0.125
- expert_ids: int32 [512, 2], P('ep'), may hold values from 0 to 7, all different within a row; in each aligned block of 128 rows (0 to 127, 128 to 255, ...) at most 48 rows name the same one
- exp_gate: bfloat16 [8, 2048, 1024], P('ep', None, 'tp'), may hold values from -0.125 to 0.125
- exp_up: bfloat16 [8, 2048, 1024], P('ep', None, 'tp'), may hold values from -0.125 to 0.125
- exp_down: bfloat16 [8, 1024, 2048], P('ep', 'tp'), may hold values from -0.1875 to 0.1875
Outputs:
- mixed: bfloat16 [512, 2048], P('ep', 'tp')
- new_matrix: float32 [512, 32, 64, 64], P('ep', 'tp')
- new_normer: float32 [512, 32, 64], P('ep', 'tp')
- new_max: float32 [512, 32], P('ep', 'tp')
The draws below stay inside these ranges and needn't reach their ends.
Inputs may be any that keep to these rules, and one draw needn't show every extreme that they name: `expert_ids`: A token's 2 experts differ. Among the 128 tokens of one index of ep (aligned blocks of rows) no expert is named more than 48 times, and in some block one expert is named exactly 48 times.
All inputs are finite; a program needn't handle non-finite values.
Results may differ from the reference program's by a relative error of at most 0.014.
Values may be sent and summed in bfloat16 or wider, within the bound.
No kernel may reach another device: no remote copies, remote signals or barrier semaphores. Data moves between devices by JAX's collectives and lax.ppermute only.
A program may use at most 128 MiB of HBM per device.

```python
import math
import jax
import jax.numpy as jnp
import numpy as np
from jax import lax

D = 2048
HEADS = 32
DK = 64
FF = 1024
N_GROUPS = 4
TOPK = 2
SEQ_GRP = 128
TOKENS = 512
EXPERTS = 8
EXP_GROUP = 2
CAP = 48
N_EP = 4


def steps_of(rng, shape, split, low, largest):
    loudness = 1.0
    for axis_at, shards_of in split:
        draws = jax.random.uniform(jax.random.fold_in(jax.random.fold_in(rng, 6), axis_at), (shards_of,), jnp.float32, low / len(split), largest / len(split))
        loudness = loudness * jnp.repeat(jnp.exp(draws), shape[axis_at] // shards_of).reshape((-1,) + (1,) * (len(shape) - 1 - axis_at))
    return loudness


def routed_block(own_key, own, number, rows, amount, top, most, slope):
    order = jax.random.permutation(own_key, amount)
    packed, usual = shares(amount, rows * top, most, slope, True), shares(amount, rows * top, most, slope, False)
    places = jnp.arange(amount)

    def named(tallies, turn):
        used = int((tallies > 0).sum())
        fixed = max(1, used // 4)
        shifted = fixed + (places - fixed + turn * (used - fixed)) % max(1, amount - fixed)
        return jnp.zeros((amount,), jnp.int32).at[order[jnp.where(places < fixed, places, shifted)]].set(jnp.asarray(tallies, jnp.int32))

    tallies = jnp.where(number % 4 == 0, named(packed, number // 4), named(usual, number - number // 4 - 1))
    mixed = jax.random.permutation(jax.random.fold_in(own, 3), amount)
    giver, receiver = mixed[0:amount // 2 * 2:2], mixed[1:amount // 2 * 2:2]
    slack = jnp.minimum(tallies[giver] - 1, most - tallies[receiver]) // 2
    slack = jnp.where((giver == order[0]) | (receiver == order[0]) | (tallies[receiver] == 0), 0, jnp.maximum(slack, 0))
    shifted = jax.random.randint(jax.random.fold_in(own, 4), (amount // 2,), 0, 1 << 20) % (slack + 1)
    tallies = tallies.at[giver].add(-shifted).at[receiver].add(shifted)
    labels = jnp.searchsorted(jnp.cumsum(tallies), jnp.arange(rows * top), side="right").astype(jnp.int32)
    grid = labels.reshape(top, rows).T
    grid = grid[jax.random.permutation(jax.random.fold_in(own, 1), rows)]
    turn = jax.random.randint(jax.random.fold_in(own, 2), (rows, 1), 0, top)
    return jnp.take_along_axis(grid, (jnp.arange(top)[None, :] + turn) % top, axis=1)


def shares(amount, total, bound, slope, full):
    loads = [(1 << 20) // math.isqrt(standing ** slope) + 1 for standing in range(1, amount + 1)]
    largest = bound if full else min(bound, max(-(-total // amount), total * loads[0] // sum(loads)))
    least = 1 if total - largest >= amount - 1 else 0
    holding, surplus = [largest] + [least] * (amount - 1), total - largest - least * (amount - 1)
    while surplus > 0:
        candidates = [i for i in range(1, amount) if holding[i] < largest] or [i for i in range(1, amount) if holding[i] < bound]
        whole, left = sum([loads[i] for i in candidates]), surplus
        for i in candidates:
            more = min(bound - holding[i], max(1, left * loads[i] // whole), surplus)
            holding[i] = holding[i] + more
            surplus = surplus - more
    return np.array(holding)


def normal_values(key, shape, spread, bound, cuts=(), kind=jnp.bfloat16):
    factor_of = steps_of(key, shape, cuts, -0.22, 0.18) if cuts else 1.0
    result = jax.random.normal(key, shape, jnp.float32) * spread * factor_of
    return jnp.minimum(jnp.maximum(result, -bound), bound).astype(kind)


def setup_inputs(seed: int = 0) -> dict:
    keys = jax.random.split(jax.random.key(seed), 22)
    resid = normal_values(keys[0], (TOKENS, D), 1.0, 6.0, ((0, 4),))
    norm1_gain = jnp.clip(1.0 + 0.18 * jax.random.normal(keys[1], (D,), jnp.float32), 0.1, 1.9)
    w_query = normal_values(keys[2], (D, HEADS * DK), D ** -0.5, 0.125, ((0, 4), (1, 8)))
    w_key = normal_values(keys[3], (D, HEADS * DK), D ** -0.5, 0.125, ((0, 4), (1, 8)))
    w_value = normal_values(keys[4], (D, HEADS * DK), D ** -0.5, 0.125, ((0, 4), (1, 8)))
    w_outgate = normal_values(keys[5], (D, HEADS * DK), D ** -0.5, 0.125, ((0, 4), (1, 8)))
    w_igate = normal_values(keys[6], (D, HEADS), D ** -0.5, 0.125)
    w_fgate = normal_values(keys[7], (D, HEADS), D ** -0.5, 0.125)
    forget_bias = jnp.clip(jax.random.uniform(keys[8], (HEADS,), jnp.float32, 0.0, 4.0), 0.0, 4.0)
    head_gain = jnp.clip(1.0 + 0.18 * jax.random.normal(keys[9], (HEADS * DK,), jnp.float32), 0.1, 1.9)
    w_out = normal_values(keys[10], (HEADS * DK, D), (HEADS * DK) ** -0.5, 0.125, ((0, 8),))
    state_matrix = normal_values(keys[11], (TOKENS, HEADS, DK, DK), 0.5, 4.0, ((0, 4), (1, 8)), jnp.float32)
    state_norm = normal_values(keys[12], (TOKENS, HEADS, DK), 2.0, 8.0, ((0, 4), (1, 8)), jnp.float32)
    state_max = jnp.clip(-1.0 + 3.0 * jax.random.uniform(keys[13], (TOKENS, HEADS), jnp.float32) ** steps_of(keys[13], (TOKENS, HEADS), ((0, 4), (1, 8)), -0.2, 0.2), -1.0, 2.0)
    norm2_gain = jnp.clip(1.0 + 0.18 * jax.random.normal(keys[14], (D,), jnp.float32), 0.1, 1.9)
    group_router = normal_values(keys[15], (D, N_GROUPS), D ** -0.5, 0.125)
    expert_router = normal_values(keys[16], (D, EXPERTS), D ** -0.5, 0.125)
    expert_ids_keys = jax.random.split(jax.random.fold_in(keys[17], 1), TOKENS // SEQ_GRP)
    expert_ids_turns = jax.random.permutation(jax.random.fold_in(keys[17], 3), TOKENS // SEQ_GRP)
    expert_ids = jax.vmap(lambda own, number: routed_block(jax.random.fold_in(keys[17], 2), own, number, SEQ_GRP, EXPERTS, TOPK, CAP, 2))(expert_ids_keys, expert_ids_turns).reshape((TOKENS, TOPK))
    exp_gate = normal_values(keys[18], (EXPERTS, D, FF), D ** -0.5, 0.125, ((0, 4), (2, 8)))
    exp_up = normal_values(keys[19], (EXPERTS, D, FF), D ** -0.5, 0.125, ((0, 4), (2, 8)))
    exp_down = normal_values(keys[20], (EXPERTS, FF, D), FF ** -0.5, 0.1875, ((0, 4), (1, 8)))
    return {"resid": resid, "norm1_gain": norm1_gain, "w_query": w_query, "w_key": w_key, "w_value": w_value, "w_outgate": w_outgate, "w_igate": w_igate, "w_fgate": w_fgate, "forget_bias": forget_bias, "head_gain": head_gain, "w_out": w_out, "state_matrix": state_matrix, "state_norm": state_norm, "state_max": state_max, "norm2_gain": norm2_gain, "group_router": group_router, "expert_router": expert_router, "expert_ids": expert_ids, "exp_gate": exp_gate, "exp_up": exp_up, "exp_down": exp_down}


EPSILON = 1e-06

def rms_scale(values, gain):
    widened = values.astype(jnp.float32)
    factor = lax.rsqrt(lax.optimization_barrier(jnp.mean(widened * widened, axis=-1, keepdims=True)) + EPSILON)
    return widened * factor * gain.astype(jnp.float32)

def memory_cell(scaled, key_rows, value_rows, in_gate, log_forget, matrix, normer, running):
    stable = jnp.maximum(log_forget + running, in_gate)
    fresh = jnp.exp(in_gate - stable)
    carried = jnp.exp(log_forget + running - stable)
    readout = jnp.einsum('bhd,bhde->bhe', scaled, matrix, precision=lax.Precision.HIGHEST)
    score = lax.optimization_barrier(jnp.sum(scaled * key_rows, axis=-1)) * fresh
    numer = carried[..., None] * readout + score[..., None] * value_rows
    denom = carried * lax.optimization_barrier(jnp.sum(scaled * normer, axis=-1)) + score
    cell_out = numer / jnp.maximum(jnp.abs(denom), 1.0)[..., None]
    new_matrix = carried[..., None, None] * matrix + fresh[..., None, None] * key_rows[..., :, None] * value_rows[..., None, :]
    new_normer = carried[..., None] * normer + fresh[..., None] * key_rows
    return (cell_out, new_matrix, new_normer, stable)

def reference(resid, norm1_gain, w_query, w_key, w_value, w_outgate, w_igate, w_fgate, forget_bias, head_gain, w_out, state_matrix, state_norm, state_max, norm2_gain, group_router, expert_router, expert_ids, exp_gate, exp_up, exp_down):
    rows = resid.shape[0]
    heads = state_matrix.shape[1]
    size = state_matrix.shape[2]
    normed = rms_scale(resid, norm1_gain).astype(jnp.bfloat16)

    def project(weight):
        product = jnp.dot(normed, weight, preferred_element_type=jnp.float32)
        stored = lax.optimization_barrier(product.astype(jnp.bfloat16))
        return stored.astype(jnp.float32).reshape(rows, heads, size)
    scaled = project(w_query) * size ** (-0.5)
    key_rows = project(w_key)
    value_rows = project(w_value)
    outgate = project(w_outgate)
    in_gate = jnp.dot(normed, w_igate, preferred_element_type=jnp.float32)
    log_forget = jax.nn.log_sigmoid(jnp.dot(normed, w_fgate, preferred_element_type=jnp.float32) + forget_bias)
    cell_out, new_matrix, new_normer, new_max = memory_cell(scaled, key_rows, value_rows, in_gate, log_forget, state_matrix, state_norm, state_max)
    headed = cell_out * lax.rsqrt(lax.optimization_barrier(jnp.mean(cell_out * cell_out, axis=-1, keepdims=True)) + EPSILON)
    headed = headed * head_gain.reshape(heads, size) * jax.nn.sigmoid(outgate)
    head_out = headed.astype(jnp.bfloat16).reshape(rows, heads * size)
    after_mix = (resid.astype(jnp.float32) + jnp.dot(head_out, w_out, preferred_element_type=jnp.float32)).astype(jnp.bfloat16)
    normed2 = rms_scale(after_mix, norm2_gain).astype(jnp.bfloat16)
    group_exp = jnp.exp(jnp.dot(normed2, group_router, preferred_element_type=jnp.float32))
    group_prob = group_exp / lax.optimization_barrier(jnp.sum(group_exp, axis=1, keepdims=True))
    expert_logits = jnp.dot(normed2, expert_router, preferred_element_type=jnp.float32)
    chosen_exp = jnp.exp(jnp.take_along_axis(expert_logits, expert_ids, axis=1))
    share = chosen_exp / lax.optimization_barrier(jnp.sum(chosen_exp, axis=1, keepdims=True))
    group_weight = jnp.take_along_axis(group_prob, expert_ids // EXP_GROUP, axis=1)
    route_weight = group_weight * share
    limit = CAP * N_EP

    def one_expert(total, inputs):
        expert_index, gate_w, up_w, down_w = inputs
        picked = expert_ids == expert_index
        coeff = lax.optimization_barrier(jnp.sum(jnp.where(picked, route_weight, 0.0), axis=1))
        member = jnp.any(picked, axis=1)
        count = jnp.sum(member.astype(jnp.int32))
        places = jnp.nonzero(member, size=limit, fill_value=0)[0].astype(jnp.int32)
        valid = (jnp.arange(limit, dtype=jnp.int32) < count).astype(jnp.float32)
        taken = normed2[places]
        gate_part = jnp.dot(taken, gate_w, preferred_element_type=jnp.float32)
        up_part = jnp.dot(taken, up_w, preferred_element_type=jnp.float32)
        units = (jax.nn.silu(gate_part) * up_part).astype(jnp.bfloat16)
        expert_out = jnp.dot(units, down_w, preferred_element_type=jnp.float32)
        total = total.at[places].add(expert_out * (coeff[places] * valid)[:, None])
        return (total, None)
    start_total = jnp.zeros((rows, resid.shape[1]), jnp.float32)
    moe, _ = lax.scan(one_expert, start_total, (jnp.arange(EXPERTS, dtype=jnp.int32), exp_gate, exp_up, exp_down))
    mixed = (after_mix.astype(jnp.float32) + moe).astype(jnp.bfloat16)
    return (mixed, new_matrix, new_normer, new_max)
```

```python
import jax
import jax.numpy as jnp
from jax import lax
from jax.sharding import PartitionSpec as P

EPSILON = 1e-06
CORES = 2


def ep_send(value, step):
    count = lax.axis_size("ep")
    return lax.ppermute(value, "ep", [(i, i ^ step) for i in range(count)])


def chip_send(value, step):
    count = lax.axis_size("tp")
    return lax.ppermute(value, "tp", [(i, i ^ (CORES * step)) for i in range(count)])


def core_send(value):
    count = lax.axis_size("tp")
    return lax.ppermute(value, "tp", [(i, i ^ 1) for i in range(count)])


def dot(lhs, rhs, lhs_dim, rhs_dim):
    return lax.dot_general(
        lhs, rhs, (((lhs_dim,), (rhs_dim,)), ((), ())), preferred_element_type=jnp.float32
    )


def per_device(
    resid,
    norm1_gain,
    w_query,
    w_key,
    w_value,
    w_outgate,
    w_igate,
    w_fgate,
    forget_bias,
    head_gain,
    w_out,
    state_matrix,
    state_norm,
    state_max,
    norm2_gain,
    group_router,
    expert_router,
    expert_ids,
    exp_gate,
    exp_up,
    exp_down,
):
    f32, bf16 = jnp.float32, jnp.bfloat16
    rows, width = resid.shape
    heads, size = state_matrix.shape[1], state_matrix.shape[2]
    ep_count, tp_count = lax.axis_size("ep"), lax.axis_size("tp")
    chips = tp_count // CORES
    ep_rank, tp_rank = lax.axis_index("ep"), lax.axis_index("tp")
    chip_rank, core_rank = tp_rank // CORES, tp_rank % CORES
    cols = width // tp_count
    depth = w_query.shape[0]
    experts_all, groups = expert_router.shape[1], group_router.shape[1]
    per_group = experts_all // groups
    topk = expert_ids.shape[1]
    local_experts = exp_gate.shape[0]
    hidden = exp_gate.shape[2]
    capacity = max(2, 3 * rows * topk // (2 * experts_all))

    def split_cols(value, axis, core):
        shape = value.shape
        value = value.reshape(shape[:axis] + (chips, CORES, cols) + shape[axis + 1 :])
        value = lax.dynamic_index_in_dim(value, core, axis + 1, keepdims=False)
        parts = [
            lax.dynamic_index_in_dim(value, chip_rank ^ k, axis, keepdims=False)
            for k in range(chips)
        ]
        return jnp.concatenate(parts, axis=axis)

    wide = resid.astype(f32)
    factor1 = lax.rsqrt(jnp.mean(wide * wide, axis=1, keepdims=True) + EPSILON)
    normed = (wide * factor1 * norm1_gain).astype(bf16)
    blocks = []
    for k in range(ep_count):
        start = (ep_rank ^ k) * depth
        piece = lax.dynamic_slice_in_dim(resid, start, depth, 1).astype(f32)
        gain = lax.dynamic_slice_in_dim(norm1_gain, start, depth, 0)
        blocks.append((piece * factor1 * gain).astype(bf16))
    blocks = [blocks[0]] + [ep_send(blocks[k], k) for k in range(1, ep_count)]
    joined = jnp.concatenate((w_query, w_key, w_value, w_outgate), axis=1)
    total = None
    sent = []
    for k in range(1, ep_count):
        sent.append(ep_send(dot(joined, blocks[k], 0, 1).astype(bf16), k))
    total = dot(joined, blocks[0], 0, 1)
    for value in sent:
        total = total + value.astype(f32)
    stored = total.astype(bf16).astype(f32).reshape(4, heads, size, rows)
    scaled = stored[0] * size ** (-0.5)
    key_rows, value_rows, outgate = stored[1], stored[2], stored[3]

    head_start = tp_rank * heads
    gate_rows = lax.dynamic_slice_in_dim(w_igate.T, head_start, heads, 0)
    forget_rows = lax.dynamic_slice_in_dim(w_fgate.T, head_start, heads, 0)
    bias = lax.dynamic_slice_in_dim(forget_bias, head_start, heads, 0)[:, None]
    both = dot(jnp.concatenate((gate_rows, forget_rows), axis=0), normed, 1, 1)
    in_gate = both[:heads]
    log_forget = jax.nn.log_sigmoid(both[heads:] + bias)
    running = log_forget + state_max.T
    new_max = jnp.maximum(running, in_gate)
    fresh = jnp.exp(in_gate - new_max)
    carried = jnp.exp(running - new_max)

    matrix = state_matrix.transpose(1, 2, 3, 0)
    normer = state_norm.transpose(1, 2, 0)
    readout = jnp.sum(scaled[:, :, None, :] * matrix, axis=1)
    score = jnp.sum(scaled * key_rows, axis=1) * fresh
    numer = carried[:, None] * readout + score[:, None] * value_rows
    denom = carried * jnp.sum(scaled * normer, axis=1) + score
    cell_out = numer / jnp.maximum(jnp.abs(denom), 1.0)[:, None]
    headed = cell_out * lax.rsqrt(jnp.mean(cell_out * cell_out, axis=1, keepdims=True) + EPSILON)
    headed = headed * head_gain.reshape(heads, size, 1) * jax.nn.sigmoid(outgate)
    head_out = headed.astype(bf16).reshape(heads * size, rows)

    w_send = split_cols(w_out, 1, 1 - core_rank)
    w_keep = split_cols(w_out, 1, core_rank)
    away = dot(head_out, w_send, 0, 0).astype(bf16)
    crossed = core_send(away)
    mix = dot(head_out, w_keep, 0, 0) + crossed.astype(f32)
    mix_parts = [mix[:, k * cols : (k + 1) * cols] for k in range(chips)]
    own_resid = lax.dynamic_slice_in_dim(resid, tp_rank * cols, cols, 1).astype(f32)
    arrived = [chip_send(mix_parts[k].astype(bf16), k) for k in range(1, chips)]

    late = lax.optimization_barrier((key_rows, value_rows, carried, fresh, away))
    new_key, new_value, new_carried, new_fresh = late[0], late[1], late[2], late[3]
    scaled_key = new_fresh[:, None] * new_key
    new_matrix = new_carried[:, None, None] * matrix + scaled_key[:, :, None] * new_value[:, None]
    new_normer = new_carried[:, None] * normer + scaled_key

    attended = mix_parts[0]
    for value in arrived:
        attended = attended + value.astype(f32)
    after_cols = (own_resid + attended).astype(bf16)
    after_parts = [after_cols] + [chip_send(after_cols, k) for k in range(1, chips)]
    after_own = jnp.concatenate(after_parts, axis=1)

    expert_range = jnp.arange(experts_all, dtype=jnp.int32)
    one_hot = (expert_ids[:, :, None] == expert_range).astype(f32)
    counts = jnp.sum(one_hot, axis=1).astype(bf16)
    before = (jnp.arange(rows)[:, None] > jnp.arange(rows)[None, :]).astype(bf16)
    earlier = dot(before, counts, 1, 0)
    slot = jnp.sum(one_hot * earlier[:, None, :], axis=2).astype(jnp.int32)
    position = (
        ((expert_ids // local_experts) ^ ep_rank) * local_experts + expert_ids % local_experts
    ) * capacity + slot
    slot_range = jnp.arange(experts_all * capacity, dtype=jnp.int32)
    matched = position[:, :, None] == slot_range
    dispatch = jnp.any(matched, axis=1).astype(bf16)

    buffer = dot(dispatch, after_own, 0, 0).astype(bf16)
    slots = local_experts * capacity
    taken = [buffer[:slots]] + [
        ep_send(buffer[k * slots : (k + 1) * slots], k) for k in range(1, ep_count)
    ]

    gain_own = split_cols(norm2_gain, 0, core_rank)
    gain_other = split_cols(norm2_gain, 0, 1 - core_rank)
    routers = split_cols(jnp.concatenate((group_router, expert_router), axis=1).T, 1, core_rank)
    after_wide = after_own.astype(f32)
    logits_part = dot((after_wide * gain_own).astype(bf16), routers, 1, 1)
    square_part = jnp.sum(after_wide * after_wide, axis=1, keepdims=True)
    route_part = jnp.concatenate((logits_part, square_part), axis=1)
    route_all = route_part + core_send(route_part)
    factor_home = lax.rsqrt(route_all[:, -1:] / width + EPSILON)
    logits = route_all[:, :-1] * factor_home
    group_exp = jnp.exp(logits[:, :groups])
    group_prob = group_exp / jnp.sum(group_exp, axis=1, keepdims=True)
    chosen_exp = jnp.exp(jnp.sum(one_hot * logits[:, None, groups:], axis=2))
    share = chosen_exp / jnp.sum(chosen_exp, axis=1, keepdims=True)
    group_hot = (
        (expert_ids // per_group)[:, :, None] == jnp.arange(groups, dtype=jnp.int32)
    ).astype(f32)
    route_weight = jnp.sum(group_hot * group_prob[:, None, :], axis=2) * share
    combine = jnp.sum(matched.astype(f32) * route_weight[:, :, None], axis=1)
    combine_high = combine.astype(bf16)
    combine_low = (combine - combine_high.astype(f32)).astype(bf16)

    gate_up = jnp.concatenate((exp_gate, exp_up), axis=2)
    in_own = (split_cols(gate_up, 1, core_rank).astype(f32) * gain_own[:, None]).astype(bf16)
    in_other = (split_cols(gate_up, 1, 1 - core_rank).astype(f32) * gain_other[:, None]).astype(bf16)
    down_keep = split_cols(exp_down, 2, core_rank)
    down_send = split_cols(exp_down, 2, 1 - core_rank)
    half = cols * chips
    own = jnp.stack(taken, 0).reshape(ep_count, local_experts, capacity, half)
    other = core_send(own)
    squares = jnp.sum(jnp.square(own.astype(f32)), axis=3, keepdims=True) + jnp.sum(
        jnp.square(other.astype(f32)), axis=3, keepdims=True
    )
    factor2 = lax.rsqrt(squares / width + EPSILON)
    inner = jnp.einsum("secd,edf->secf", own, in_own, preferred_element_type=f32) + jnp.einsum(
        "secd,edf->secf", other, in_other, preferred_element_type=f32
    )
    inner = inner * factor2
    units = (jax.nn.silu(inner[..., :hidden]) * inner[..., hidden:]).astype(bf16)
    terms_send = jnp.einsum("secf,efd->secd", units, down_send, preferred_element_type=f32)
    terms_crossed = core_send(terms_send.astype(bf16))
    terms_keep = jnp.einsum("secf,efd->secd", units, down_keep, preferred_element_type=f32)
    terms = (terms_keep + terms_crossed.astype(f32)).astype(bf16)
    terms = terms.reshape(ep_count, slots, half)
    back = jnp.concatenate([terms[0]] + [ep_send(terms[k], k) for k in range(1, ep_count)], 0)
    moe = dot(combine_high, back, 1, 0) + dot(combine_low, back, 1, 0)
    moe_parts = [moe[:, k * cols : (k + 1) * cols] for k in range(chips)]
    moe_got = [chip_send(moe_parts[k].astype(bf16), k) for k in range(1, chips)]
    final = after_cols.astype(f32) + moe_parts[0]
    for value in moe_got:
        final = final + value.astype(f32)
    return (
        final.astype(bf16),
        new_matrix.transpose(3, 0, 1, 2),
        new_normer.transpose(2, 0, 1),
        new_max.T,
    )


def solution(mesh):
    in_specs = (
        P("ep", None),
        P(),
        P("ep", "tp"),
        P("ep", "tp"),
        P("ep", "tp"),
        P("ep", "tp"),
        P(),
        P(),
        P(),
        P("tp"),
        P("tp", None),
        P("ep", "tp", None, None),
        P("ep", "tp", None),
        P("ep", "tp"),
        P(),
        P(),
        P(),
        P("ep", None),
        P("ep", None, "tp"),
        P("ep", None, "tp"),
        P("ep", "tp", None),
    )
    out_specs = (P("ep", "tp"), P("ep", "tp", None, None), P("ep", "tp", None), P("ep", "tp"))
    return jax.shard_map(
        per_device, mesh=mesh, in_specs=in_specs, out_specs=out_specs, check_vma=False
    )
```

```python
import functools

import jax
import jax.numpy as jnp
from jax import lax
from jax.experimental import pallas as pl
from jax.experimental.pallas import tpu as pltpu
from jax.sharding import PartitionSpec as P

EPSILON = 1e-06
CORES = 2
VMEM = pltpu.MemorySpace.VMEM
F32, BF16 = jnp.float32, jnp.bfloat16


def ep_send(value, step):
    count = lax.axis_size("ep")
    return lax.ppermute(value, "ep", [(i, i ^ step) for i in range(count)])


def chip_send(value, step):
    count = lax.axis_size("tp")
    return lax.ppermute(value, "tp", [(i, i ^ (CORES * step)) for i in range(count)])


def core_send(value):
    count = lax.axis_size("tp")
    return lax.ppermute(value, "tp", [(i, i ^ 1) for i in range(count)])


def dot(lhs, rhs, lhs_dim, rhs_dim):
    return lax.dot_general(
        lhs, rhs, (((lhs_dim,), (rhs_dim,)), ((), ())), preferred_element_type=F32
    )


def call(kernel, name, outs, *args, limit=None):
    return pl.pallas_call(
        kernel,
        name=name,
        out_shape=[jax.ShapeDtypeStruct(shape, dtype) for shape, dtype in outs],
        in_specs=[pl.BlockSpec(memory_space=VMEM) for _ in args],
        out_specs=[pl.BlockSpec(memory_space=VMEM) for _ in outs],
        compiler_params=pltpu.CompilerParams(vmem_limit_bytes=limit or 48 << 20),
    )(*args)


def block_cols(step, core, cols):
    chip = (lax.axis_index("tp") // CORES) ^ step
    return pl.ds(pl.multiple_of((chip * CORES + core) * cols, cols), cols)


def norm_kernel(steps, depth, resid_ref, gain_ref, normed_ref, *block_refs):
    width = resid_ref.shape[1]
    wide = resid_ref[...].astype(F32)
    factor = lax.rsqrt(jnp.sum(wide * wide, axis=1, keepdims=True) / width + EPSILON)
    normed_ref[...] = (wide * factor * gain_ref[...]).astype(BF16)
    for step, block_ref in zip(steps, block_refs):
        start = pl.multiple_of((lax.axis_index("ep") ^ step) * depth, depth)
        block_ref[...] = normed_ref[:, pl.ds(start, depth)]


def project_kernel(x_ref, *refs):
    weights, out_ref = refs[:-1], refs[-1]
    cols = weights[0].shape[1]
    for i, w_ref in enumerate(weights):
        out_ref[:, i * cols : (i + 1) * cols] = jnp.dot(
            x_ref[...], w_ref[...], preferred_element_type=F32
        ).astype(out_ref.dtype)


def cell_kernel(heads, size, chips, cols, received, *refs):
    own_ref = refs[0]
    got_refs = refs[1 : 1 + received]
    (gates_ref, matrix_ref, normer_ref, gain_ref, w_ref) = refs[1 + received : 6 + received]
    away_ref, keep_ref, key_ref, value_ref, norm_ref, turned_ref = refs[6 + received :]
    total = own_ref[...]
    for ref in got_refs:
        total = total + ref[...].astype(F32)
    turned_ref[...] = total.astype(BF16).astype(F32).T
    span = heads * size
    outs = []
    for h in range(heads):
        carried = gates_ref[h : h + 1, :]
        fresh = gates_ref[heads + h : heads + h + 1, :]
        scaled = turned_ref[h * size : (h + 1) * size, :] * size ** (-0.5)
        keys = turned_ref[span + h * size : span + (h + 1) * size, :]
        values = turned_ref[2 * span + h * size : 2 * span + (h + 1) * size, :]
        outgate = turned_ref[3 * span + h * size : 3 * span + (h + 1) * size, :]
        normer = normer_ref[h]
        readout = scaled[0:1, :] * matrix_ref[h, 0]
        for d in range(1, size):
            readout = readout + scaled[d : d + 1, :] * matrix_ref[h, d]
        score = jnp.sum(scaled * keys, axis=0, keepdims=True) * fresh
        numer = carried * readout + score * values
        denom = carried * jnp.sum(scaled * normer, axis=0, keepdims=True) + score
        cell = numer / jnp.maximum(jnp.abs(denom), 1.0)
        cell = cell * lax.rsqrt(jnp.mean(cell * cell, axis=0, keepdims=True) + EPSILON)
        gain = gain_ref[h * size : (h + 1) * size, :]
        outs.append((cell * gain * jax.nn.sigmoid(outgate)).astype(BF16))
        key_ref[h] = keys
        value_ref[h] = values
        norm_ref[h] = carried * normer + fresh * keys
    head_out = jnp.concatenate(outs, axis=0).astype(F32).T.astype(BF16)
    core = lax.axis_index("tp") % CORES
    for k in range(chips):
        at = slice(k * cols, (k + 1) * cols)
        away_ref[:, at] = jnp.dot(
            head_out, w_ref[:, block_cols(k, 1 - core, cols)], preferred_element_type=F32
        ).astype(BF16)
        keep_ref[:, at] = jnp.dot(
            head_out, w_ref[:, block_cols(k, core, cols)], preferred_element_type=F32
        )


def dispatch_kernel(chips, cols, capacity, *refs):
    own_refs = refs[:chips]
    other_ref, gain_ref, pick_ref = refs[chips : chips + 3]
    normed_ref, out_refs, full_ref = refs[chips + 3], refs[chips + 4 : -1], refs[-1]
    core = lax.axis_index("tp") % CORES
    for k in range(chips):
        full_ref[:, block_cols(k, core, cols)] = own_refs[k][...].astype(F32)
        full_ref[:, block_cols(k, 1 - core, cols)] = other_ref[
            :, k * cols : (k + 1) * cols
        ].astype(F32)
    full = full_ref[...]
    factor = lax.rsqrt(jnp.sum(full * full, axis=1, keepdims=True) / full.shape[1] + EPSILON)
    normed = (full * factor * gain_ref[...]).astype(BF16)
    normed_ref[...] = normed
    picked = jnp.dot(pick_ref[...], normed, preferred_element_type=F32)
    for k, out_ref in enumerate(out_refs):
        out_ref[...] = picked[k * capacity : (k + 1) * capacity].astype(BF16)


def expert_kernel(blocks, *refs):
    x_refs = refs[:blocks]
    weights = refs[blocks : blocks + 6]
    out_refs = refs[blocks + 6 :]
    x = jnp.concatenate([ref[...] for ref in x_refs], axis=0)
    result = None
    for gate_ref, up_ref, down_ref in (weights[:3], weights[3:]):
        gate = jnp.dot(x, gate_ref[...], preferred_element_type=F32)
        up = jnp.dot(x, up_ref[...], preferred_element_type=F32)
        units = (jax.nn.silu(gate) * up).astype(BF16)
        part = jnp.dot(units, down_ref[...], preferred_element_type=F32)
        result = part if result is None else result + part
    capacity = x_refs[0].shape[0]
    for k, out_ref in enumerate(out_refs):
        out_ref[...] = result[k * capacity : (k + 1) * capacity].astype(BF16)


def combine_kernel(chips, cols, blocks, *refs):
    y_refs = refs[:blocks]
    high_ref, low_ref, away_ref, keep_ref = refs[blocks:]
    core = lax.axis_index("tp") % CORES
    for k in range(chips):
        at = slice(k * cols, (k + 1) * cols)
        for target, out_ref in ((1 - core, away_ref), (core, keep_ref)):
            ds = block_cols(k, target, cols)
            y = jnp.concatenate([ref[:, ds] for ref in y_refs], axis=0)
            value = jnp.dot(high_ref[...], y, preferred_element_type=F32)
            value = value + jnp.dot(low_ref[...], y, preferred_element_type=F32)
            out_ref[:, at] = value.astype(out_ref.dtype)


def per_device(
    resid,
    norm1_gain,
    w_query,
    w_key,
    w_value,
    w_outgate,
    w_igate,
    w_fgate,
    forget_bias,
    head_gain,
    w_out,
    state_matrix,
    state_norm,
    state_max,
    norm2_gain,
    group_router,
    expert_router,
    expert_ids,
    exp_gate,
    exp_up,
    exp_down,
):
    rows, width = resid.shape
    heads, size = state_matrix.shape[1], state_matrix.shape[2]
    ep_count, tp_count = lax.axis_size("ep"), lax.axis_size("tp")
    chips = tp_count // CORES
    ep_rank, tp_rank = lax.axis_index("ep"), lax.axis_index("tp")
    core_rank = tp_rank % CORES
    cols = width // tp_count
    depth = w_query.shape[0]
    experts_all, groups = expert_router.shape[1], group_router.shape[1]
    per_group = experts_all // groups
    topk = expert_ids.shape[1]
    local_experts, _, hidden = exp_gate.shape
    assert local_experts == CORES
    capacity = max(2, 3 * rows * topk // (2 * experts_all))
    half = chips * cols
    others = range(1, ep_count)

    normed, *blocks = call(
        functools.partial(norm_kernel, range(ep_count), depth),
        "first_norm",
        [((rows, width), BF16)] + [((rows, depth), BF16)] * ep_count,
        resid,
        norm1_gain[None, :],
    )
    weights = (w_query, w_key, w_value, w_outgate)
    span = 4 * heads * size
    arrived = [ep_send(blocks[k], k) for k in others]
    (own,) = call(project_kernel, "project_own", [((rows, span), F32)], blocks[0], *weights)
    sent = []
    for k in others:
        (part,) = call(
            project_kernel, f"project_{k}", [((rows, span), BF16)], arrived[k - 1], *weights
        )
        sent.append(ep_send(part, k))

    def swap(value):
        mine = lax.dynamic_index_in_dim(value, core_rank, 0, keepdims=False)
        theirs = lax.dynamic_index_in_dim(value, 1 - core_rank, 0, keepdims=False)
        return mine, core_send(theirs)

    gate_mine, gate_got = swap(exp_gate)
    up_mine, up_got = swap(exp_up)
    down_mine, down_got = swap(exp_down)

    head_start = tp_rank * heads
    gate_rows = lax.dynamic_slice_in_dim(w_igate.T, head_start, heads, 0)
    forget_rows = lax.dynamic_slice_in_dim(w_fgate.T, head_start, heads, 0)
    bias = lax.dynamic_slice_in_dim(forget_bias, head_start, heads, 0)[:, None]
    both = dot(jnp.concatenate((gate_rows, forget_rows), axis=0), normed, 1, 1)
    in_gate = both[:heads]
    running = jax.nn.log_sigmoid(both[heads:] + bias) + state_max.T
    new_max = jnp.maximum(running, in_gate)
    fresh = jnp.exp(in_gate - new_max)
    carried = jnp.exp(running - new_max)

    matrix = state_matrix.transpose(1, 2, 3, 0)
    normer = state_norm.transpose(1, 2, 0)
    cell = functools.partial(cell_kernel, heads, size, chips, cols, ep_count - 1)
    away, keep, key_rows, value_rows, new_normer = pl.pallas_call(
        cell,
        name="cell",
        out_shape=[
            jax.ShapeDtypeStruct((rows, half), BF16),
            jax.ShapeDtypeStruct((rows, half), F32),
            jax.ShapeDtypeStruct((heads, size, rows), F32),
            jax.ShapeDtypeStruct((heads, size, rows), F32),
            jax.ShapeDtypeStruct((heads, size, rows), F32),
        ],
        in_specs=[pl.BlockSpec(memory_space=VMEM)] * (ep_count + 5),
        out_specs=[pl.BlockSpec(memory_space=VMEM)] * 5,
        scratch_shapes=[pltpu.VMEM((span, rows), F32)],
        compiler_params=pltpu.CompilerParams(vmem_limit_bytes=48 << 20),
    )(
        own,
        *sent,
        jnp.concatenate((carried, fresh), axis=0),
        matrix,
        normer,
        jnp.broadcast_to(head_gain[:, None], (heads * size, rows)),
        w_out,
    )

    mix = keep + core_send(away).astype(F32)
    mix_parts = [mix[:, k * cols : (k + 1) * cols] for k in range(chips)]
    own_resid = lax.dynamic_slice_in_dim(resid, tp_rank * cols, cols, 1).astype(F32)
    mix_got = [chip_send(mix_parts[k].astype(BF16), k) for k in range(1, chips)]

    scaled_key = fresh[:, None] * key_rows
    new_matrix = carried[:, None, None] * matrix + scaled_key[:, :, None] * value_rows[:, None]

    attended = mix_parts[0]
    for value in mix_got:
        attended = attended + value.astype(F32)
    after_cols = (own_resid + attended).astype(BF16)
    after_parts = [after_cols] + [chip_send(after_cols, k) for k in range(1, chips)]
    after_other = core_send(jnp.concatenate(after_parts, axis=1))

    expert_range = jnp.arange(experts_all, dtype=jnp.int32)
    one_hot = (expert_ids[:, :, None] == expert_range).astype(F32)
    counts = jnp.sum(one_hot, axis=1).astype(BF16)
    before = (jnp.arange(rows)[:, None] > jnp.arange(rows)[None, :]).astype(BF16)
    earlier = dot(before, counts, 1, 0)
    slot = jnp.sum(one_hot * earlier[:, None, :], axis=2).astype(jnp.int32)
    position = ((expert_ids // local_experts) ^ ep_rank) * capacity + slot
    position = jnp.where(expert_ids % local_experts == core_rank, position, -1)
    slot_range = jnp.arange(ep_count * capacity, dtype=jnp.int32)
    matched = position[:, :, None] == slot_range
    picks = jnp.any(position.T[:, None, :] == slot_range[:, None], axis=0).astype(BF16)

    normed2, *buffers = pl.pallas_call(
        functools.partial(dispatch_kernel, chips, cols, capacity),
        name="dispatch",
        out_shape=[jax.ShapeDtypeStruct((rows, width), BF16)]
        + [jax.ShapeDtypeStruct((capacity, width), BF16)] * ep_count,
        in_specs=[pl.BlockSpec(memory_space=VMEM)] * (chips + 3),
        out_specs=[pl.BlockSpec(memory_space=VMEM)] * (ep_count + 1),
        scratch_shapes=[pltpu.VMEM((rows, width), F32)],
        compiler_params=pltpu.CompilerParams(vmem_limit_bytes=48 << 20),
    )(*after_parts, after_other, norm2_gain[None, :], picks)
    taken = [buffers[0]] + [ep_send(buffers[k], k) for k in others]

    group_exp = jnp.exp(dot(normed2, group_router, 1, 0))
    group_prob = group_exp / jnp.sum(group_exp, axis=1, keepdims=True)
    logits = dot(normed2, expert_router, 1, 0)
    chosen_exp = jnp.exp(jnp.sum(one_hot * logits[:, None, :], axis=2))
    share = chosen_exp / jnp.sum(chosen_exp, axis=1, keepdims=True)
    group_hot = (
        (expert_ids // per_group)[:, :, None] == jnp.arange(groups, dtype=jnp.int32)
    ).astype(F32)
    route_weight = jnp.sum(group_hot * group_prob[:, None, :], axis=2) * share
    combine = jnp.sum(matched.astype(F32) * route_weight[:, :, None], axis=1)
    combine_high = combine.astype(BF16)
    combine_low = (combine - combine_high.astype(F32)).astype(BF16)

    terms = call(
        functools.partial(expert_kernel, ep_count),
        "experts",
        [((capacity, width), BF16)] * ep_count,
        *taken,
        gate_mine,
        up_mine,
        down_mine,
        gate_got,
        up_got,
        down_got,
    )
    back = [terms[0]] + [ep_send(terms[k], k) for k in others]
    moe_away, moe_keep = call(
        functools.partial(combine_kernel, chips, cols, ep_count),
        "combine",
        [((rows, half), BF16), ((rows, half), F32)],
        *back,
        combine_high,
        combine_low,
    )
    moe = moe_keep + core_send(moe_away).astype(F32)
    moe_parts = [moe[:, k * cols : (k + 1) * cols] for k in range(chips)]
    moe_got = [chip_send(moe_parts[k].astype(BF16), k) for k in range(1, chips)]
    final = after_cols.astype(F32) + moe_parts[0]
    for value in moe_got:
        final = final + value.astype(F32)
    return (
        final.astype(BF16),
        new_matrix.transpose(3, 0, 1, 2),
        new_normer.transpose(2, 0, 1),
        new_max.T,
    )


def solution(mesh):
    in_specs = (
        P("ep", None),
        P(),
        P("ep", "tp"),
        P("ep", "tp"),
        P("ep", "tp"),
        P("ep", "tp"),
        P(),
        P(),
        P(),
        P("tp"),
        P("tp", None),
        P("ep", "tp", None, None),
        P("ep", "tp", None),
        P("ep", "tp"),
        P(),
        P(),
        P(),
        P("ep", None),
        P("ep", None, "tp"),
        P("ep", None, "tp"),
        P("ep", "tp", None),
    )
    out_specs = (P("ep", "tp"), P("ep", "tp", None, None), P("ep", "tp", None), P("ep", "tp"))
    return jax.shard_map(
        per_device, mesh=mesh, in_specs=in_specs, out_specs=out_specs, check_vma=False
    )
```

```python
import functools

import jax
import jax.numpy as jnp
from jax import lax
from jax.experimental import pallas as pl
from jax.experimental.pallas import tpu as pltpu
from jax.sharding import PartitionSpec as P

EPSILON = 1e-06
CORES = 2
VMEM = pltpu.MemorySpace.VMEM
F32, BF16 = jnp.float32, jnp.bfloat16


def ep_send(value, step):
    count = lax.axis_size("ep")
    return lax.ppermute(value, "ep", [(i, i ^ step) for i in range(count)])


def chip_send(value, step):
    count = lax.axis_size("tp")
    return lax.ppermute(value, "tp", [(i, i ^ (CORES * step)) for i in range(count)])


def core_send(value):
    count = lax.axis_size("tp")
    return lax.ppermute(value, "tp", [(i, i ^ 1) for i in range(count)])


def dot(lhs, rhs, lhs_dim, rhs_dim):
    return lax.dot_general(
        lhs, rhs, (((lhs_dim,), (rhs_dim,)), ((), ())), preferred_element_type=F32
    )


def call(kernel, name, outs, *args, far=(), unread=(), far_out=(), scratch=(), limit=8):
    args = [
        pltpu.with_memory_space_constraint(value, pltpu.MemorySpace.HBM) if i in far else value
        for i, value in enumerate(args)
    ]
    return pl.pallas_call(
        kernel,
        name=name,
        out_shape=[jax.ShapeDtypeStruct(shape, dtype) for shape, dtype in outs],
        in_specs=[
            pl.BlockSpec(memory_space=pl.ANY if i in far or i in unread else VMEM)
            for i in range(len(args))
        ],
        out_specs=[
            pl.BlockSpec(memory_space=pl.ANY if i in far_out else VMEM) for i in range(len(outs))
        ],
        scratch_shapes=list(scratch),
        compiler_params=pltpu.CompilerParams(vmem_limit_bytes=limit << 20),
    )(*args)


def block_cols(step, core, cols):
    chip = (lax.axis_index("tp") // CORES) ^ step
    return pl.ds(pl.multiple_of((chip * CORES + core) * cols, cols), cols)


def norm_kernel(steps, depth, cols, resid_ref, gain_ref, normed_ref, own_ref, *refs):
    block_refs, (rows_ref, row_ref, sems) = refs[:-3], refs[-3:]
    copies = [
        pltpu.make_async_copy(resid_ref, rows_ref, sems.at[0]),
        pltpu.make_async_copy(gain_ref, row_ref, sems.at[1]),
    ]
    for copy in copies:
        copy.start()
    for copy in copies:
        copy.wait()
    width = rows_ref.shape[1]
    wide = rows_ref[...].astype(F32)
    factor = lax.rsqrt(jnp.sum(wide * wide, axis=1, keepdims=True) / width + EPSILON)
    normed_ref[...] = (wide * factor * row_ref[...]).astype(BF16)
    for step, block_ref in zip(steps, block_refs):
        start = pl.multiple_of((lax.axis_index("ep") ^ step) * depth, depth)
        block_ref[...] = normed_ref[:, pl.ds(start, depth)]
    start = pl.multiple_of(lax.axis_index("tp") * cols, cols)
    own_ref[...] = rows_ref[:, pl.ds(start, cols)].astype(F32)


def stage_kernel(heads, count, normed_ref, igate_ref, fgate_ref, bias_ref, max_ref, *refs):
    sources, outs = refs[:count], refs[count : 2 * count]
    gates_ref, new_max_ref, both_ref, sems = refs[2 * count :]
    copies = [
        pltpu.make_async_copy(source, out, sems.at[i])
        for i, (source, out) in enumerate(zip(sources, outs))
    ]
    for copy in copies:
        copy.start()
    all_heads = igate_ref.shape[0]
    both_ref[:all_heads] = dot(igate_ref[...], normed_ref[...], 1, 1)
    both_ref[all_heads:] = dot(fgate_ref[...], normed_ref[...], 1, 1) + bias_ref[...]
    start = lax.axis_index("tp") * heads
    in_gate = both_ref[pl.ds(start, heads)]
    forget = both_ref[pl.ds(all_heads + start, heads)]
    log_forget = jnp.minimum(forget, 0.0) - jnp.log1p(jnp.exp(-jnp.abs(forget)))
    running = log_forget + max_ref[...]
    new_max = jnp.maximum(running, in_gate)
    new_max_ref[...] = new_max
    gates_ref[:heads] = jnp.exp(running - new_max)
    gates_ref[heads:] = jnp.exp(in_gate - new_max)
    for copy in copies:
        copy.wait()


def swap_kernel(count, experts, after_ref, ids_ref, *refs):
    sources, outs = refs[:count], refs[count:-3]
    picks_ref, at_ref, sems = refs[-3:]
    core = lax.axis_index("tp") % CORES
    copies = []
    for i, source in enumerate(sources):
        for j, index in enumerate((core, 1 - core)):
            at = 2 * i + j
            copies.append(pltpu.make_async_copy(source.at[index], outs[at], sems.at[at]))
    for copy in copies:
        copy.start()
    topk, rows = ids_ref.shape
    slots = picks_ref.shape[0]
    local = sources[0].shape[0]
    capacity = slots // (experts // local)
    expert_iota = lax.broadcasted_iota(jnp.int32, (experts, rows), 0)
    hots = [(expert_iota == ids_ref[j : j + 1, :]).astype(F32) for j in range(topk)]
    before = lax.broadcasted_iota(jnp.int32, (rows, rows), 0) < lax.broadcasted_iota(
        jnp.int32, (rows, rows), 1
    )
    total = functools.reduce(lambda x, y: x + y, hots)
    earlier = dot(total.astype(BF16), before.astype(F32).astype(BF16), 1, 0)
    slot_iota = lax.broadcasted_iota(jnp.int32, (slots, rows), 0)
    picked = jnp.zeros((slots, rows), F32)
    for j in range(topk):
        ids = ids_ref[j : j + 1, :]
        slot = jnp.sum(earlier * hots[j], axis=0, keepdims=True).astype(jnp.int32)
        place = lax.shift_right_logical(ids, local.bit_length() - 1) ^ lax.axis_index("ep")
        at = jnp.where((ids & (local - 1)) == core, place * capacity + slot, -1)
        at_ref[j : j + 1, :] = at
        picked = picked + (slot_iota == at).astype(F32)
    picks_ref[...] = picked.astype(BF16)
    for copy in copies:
        copy.wait()


def update_kernel(heads, size, after_ref, matrix_ref, key_ref, value_ref, gates_ref, *refs):
    out_ref, done_ref, slots_ref, sems = refs
    copies = []
    for h in range(heads):
        slot = h % 2
        if h >= 2:
            copies[h - 2].wait()
        carried = gates_ref[h : h + 1, :]
        keys = key_ref[h] * gates_ref[heads + h : heads + h + 1, :]
        values = value_ref[h]
        for d in range(size):
            slots_ref[slot, d] = carried * matrix_ref[h, d] + keys[d : d + 1, :] * values
        copies.append(pltpu.make_async_copy(slots_ref.at[slot], out_ref.at[h], sems.at[slot]))
        copies[h].start()
    for copy in copies[-2:]:
        copy.wait()
    done_ref[...] = jnp.zeros_like(done_ref)


def project_kernel(x_ref, *refs):
    weights, out_ref = refs[:-1], refs[-1]
    cols = weights[0].shape[1]
    for i, w_ref in enumerate(weights):
        out_ref[:, i * cols : (i + 1) * cols] = jnp.dot(
            x_ref[...], w_ref[...], preferred_element_type=F32
        ).astype(out_ref.dtype)


def cell_kernel(heads, size, chips, cols, received, *refs):
    own_ref = refs[0]
    got_refs = refs[1 : 1 + received]
    (gates_ref, matrix_ref, normer_ref, gain_ref, w_ref) = refs[1 + received : 6 + received]
    away_ref, keep_ref, key_ref, value_ref, norm_ref, turned_ref = refs[7 + received :]
    total = own_ref[...]
    for ref in got_refs:
        total = total + ref[...].astype(F32)
    turned_ref[...] = total.astype(BF16).astype(F32).T
    span = heads * size
    outs = []
    for h in range(heads):
        carried = gates_ref[h : h + 1, :]
        fresh = gates_ref[heads + h : heads + h + 1, :]
        scaled = turned_ref[h * size : (h + 1) * size, :] * size ** (-0.5)
        keys = turned_ref[span + h * size : span + (h + 1) * size, :]
        values = turned_ref[2 * span + h * size : 2 * span + (h + 1) * size, :]
        outgate = turned_ref[3 * span + h * size : 3 * span + (h + 1) * size, :]
        normer = normer_ref[h]
        readout = scaled[0:1, :] * matrix_ref[h, 0]
        for d in range(1, size):
            readout = readout + scaled[d : d + 1, :] * matrix_ref[h, d]
        score = jnp.sum(scaled * keys, axis=0, keepdims=True) * fresh
        numer = carried * readout + score * values
        denom = carried * jnp.sum(scaled * normer, axis=0, keepdims=True) + score
        cell = numer / jnp.maximum(jnp.abs(denom), 1.0)
        cell = cell * lax.rsqrt(jnp.mean(cell * cell, axis=0, keepdims=True) + EPSILON)
        gain = gain_ref[h * size : (h + 1) * size, :]
        outs.append((cell * gain * jax.nn.sigmoid(outgate)).astype(BF16))
        key_ref[h] = keys
        value_ref[h] = values
        norm_ref[h] = carried * normer + fresh * keys
    head_out = jnp.concatenate(outs, axis=0).astype(F32).T.astype(BF16)
    core = lax.axis_index("tp") % CORES
    for k in range(chips):
        at = slice(k * cols, (k + 1) * cols)
        away_ref[:, at] = jnp.dot(
            head_out, w_ref[:, block_cols(k, 1 - core, cols)], preferred_element_type=F32
        ).astype(BF16)
        keep_ref[:, at] = jnp.dot(
            head_out, w_ref[:, block_cols(k, core, cols)], preferred_element_type=F32
        )


def after_kernel(done_ref, *refs):
    total = refs[0][...]
    for ref in refs[1:-1]:
        total = total + ref[...].astype(F32)
    refs[-1][...] = total.astype(BF16)


def route_kernel(per_group, normed_ref, group_ref, expert_ref, ids_ref, at_ref, *refs):
    high_ref, low_ref = refs
    rows, slots = high_ref.shape
    groups, experts = group_ref.shape[0], expert_ref.shape[0]
    group_exp = jnp.exp(dot(group_ref[...], normed_ref[...], 1, 1))
    group_prob = group_exp / jnp.sum(group_exp, axis=0, keepdims=True)
    logits = dot(expert_ref[...], normed_ref[...], 1, 1)
    expert_iota = lax.broadcasted_iota(jnp.int32, (experts, rows), 0)
    group_iota = lax.broadcasted_iota(jnp.int32, (groups, rows), 0)
    slot_iota = lax.broadcasted_iota(jnp.int32, (slots, rows), 0)
    chosen, shares = [], []
    for j in range(ids_ref.shape[0]):
        ids = ids_ref[j : j + 1, :]
        hot = expert_iota == ids
        chosen.append(jnp.exp(jnp.sum(jnp.where(hot, logits, 0.0), axis=0, keepdims=True)))
        first = group_iota * per_group
        hot = (first <= ids) & (ids < first + per_group)
        shares.append(jnp.sum(jnp.where(hot, group_prob, 0.0), axis=0, keepdims=True))
    total = functools.reduce(lambda x, y: x + y, chosen)
    combine = jnp.zeros((slots, rows), F32)
    for j, (value, share) in enumerate(zip(chosen, shares)):
        weight = share * value / total
        combine = combine + jnp.where(slot_iota == at_ref[j : j + 1, :], weight, 0.0)
    combine = combine.T
    high = combine.astype(BF16)
    high_ref[...] = high
    low_ref[...] = (combine - high.astype(F32)).astype(BF16)


def dispatch_kernel(chips, cols, capacity, *refs):
    own_refs = refs[:chips]
    other_ref, gain_ref, pick_ref = refs[chips : chips + 3]
    normed_ref, out_refs, full_ref = refs[chips + 3], refs[chips + 4 : -1], refs[-1]
    core = lax.axis_index("tp") % CORES
    for k in range(chips):
        full_ref[:, block_cols(k, core, cols)] = own_refs[k][...].astype(F32)
        full_ref[:, block_cols(k, 1 - core, cols)] = other_ref[
            :, k * cols : (k + 1) * cols
        ].astype(F32)
    full = full_ref[...]
    factor = lax.rsqrt(jnp.sum(full * full, axis=1, keepdims=True) / full.shape[1] + EPSILON)
    normed = (full * factor * gain_ref[...]).astype(BF16)
    normed_ref[...] = normed
    picked = jnp.dot(pick_ref[...], normed, preferred_element_type=F32)
    for k, out_ref in enumerate(out_refs):
        out_ref[...] = picked[k * capacity : (k + 1) * capacity].astype(BF16)


def expert_kernel(blocks, *refs):
    x_refs = refs[:blocks]
    weights = refs[blocks : blocks + 6]
    out_refs = refs[blocks + 6 :]
    x = jnp.concatenate([ref[...] for ref in x_refs], axis=0)
    result = None
    for gate_ref, up_ref, down_ref in (weights[:3], weights[3:]):
        gate = jnp.dot(x, gate_ref[...], preferred_element_type=F32)
        up = jnp.dot(x, up_ref[...], preferred_element_type=F32)
        units = (jax.nn.silu(gate) * up).astype(BF16)
        part = jnp.dot(units, down_ref[...], preferred_element_type=F32)
        result = part if result is None else result + part
    capacity = x_refs[0].shape[0]
    for k, out_ref in enumerate(out_refs):
        out_ref[...] = result[k * capacity : (k + 1) * capacity].astype(BF16)


def combine_kernel(chips, cols, blocks, *refs):
    y_refs = refs[:blocks]
    high_ref, low_ref, away_ref, keep_ref = refs[blocks:]
    core = lax.axis_index("tp") % CORES
    for k in range(chips):
        at = slice(k * cols, (k + 1) * cols)
        for target, out_ref in ((1 - core, away_ref), (core, keep_ref)):
            ds = block_cols(k, target, cols)
            y = jnp.concatenate([ref[:, ds] for ref in y_refs], axis=0)
            value = jnp.dot(high_ref[...], y, preferred_element_type=F32)
            value = value + jnp.dot(low_ref[...], y, preferred_element_type=F32)
            out_ref[:, at] = value.astype(out_ref.dtype)


def per_device(
    resid,
    norm1_gain,
    w_query,
    w_key,
    w_value,
    w_outgate,
    w_igate,
    w_fgate,
    forget_bias,
    head_gain,
    w_out,
    state_matrix,
    state_norm,
    state_max,
    norm2_gain,
    group_router,
    expert_router,
    expert_ids,
    exp_gate,
    exp_up,
    exp_down,
):
    rows, width = resid.shape
    heads, size = state_matrix.shape[1], state_matrix.shape[2]
    ep_count, tp_count = lax.axis_size("ep"), lax.axis_size("tp")
    chips = tp_count // CORES
    cols = width // tp_count
    depth = w_query.shape[0]
    experts_all, groups = expert_router.shape[1], group_router.shape[1]
    per_group = experts_all // groups
    topk = expert_ids.shape[1]
    local_experts, _, hidden = exp_gate.shape
    assert local_experts == CORES
    capacity = max(2, 3 * rows * topk // (2 * experts_all))
    half = chips * cols
    others = range(1, ep_count)

    normed, own_resid, *blocks = call(
        functools.partial(norm_kernel, range(ep_count), depth, cols),
        "first_norm",
        [((rows, width), BF16), ((rows, cols), F32)] + [((rows, depth), BF16)] * ep_count,
        resid,
        norm1_gain[None, :],
        far=(0, 1),
        scratch=[
            pltpu.VMEM((rows, width), BF16),
            pltpu.VMEM((1, width), F32),
            pltpu.SemaphoreType.DMA((2,)),
        ],
    )
    arrived = [ep_send(blocks[k], k) for k in others]
    matrix = state_matrix.transpose(1, 2, 3, 0)
    normer = state_norm.transpose(1, 2, 0)
    staged = (w_query, w_key, w_value, w_outgate, w_out, matrix, normer)
    all_heads = w_igate.shape[1]
    *staged, gates, new_max = call(
        functools.partial(stage_kernel, heads, len(staged)),
        "stage",
        [(value.shape, value.dtype) for value in staged]
        + [((2 * heads, rows), F32), ((heads, rows), F32)],
        normed,
        w_igate.T,
        w_fgate.T,
        jnp.broadcast_to(forget_bias[:, None], (all_heads, rows)),
        state_max.T,
        *staged,
        far=range(5, 5 + len(staged)),
        scratch=[
            pltpu.VMEM((2 * all_heads, rows), F32),
            pltpu.SemaphoreType.DMA((len(staged),)),
        ],
        limit=16,
    )
    weights, (w_out, matrix, normer) = staged[:4], staged[4:]
    span = 4 * heads * size
    (own,) = call(project_kernel, "project_own", [((rows, span), F32)], blocks[0], *weights)
    sent = []
    for k in others:
        (part,) = call(
            project_kernel, f"project_{k}", [((rows, span), BF16)], arrived[k - 1], *weights
        )
        sent.append(ep_send(part, k))
        sent_last = part

    pair = (exp_gate, exp_up, exp_down)
    slots = ep_count * capacity
    *mine_and_theirs, picks, places = call(
        functools.partial(swap_kernel, len(pair), experts_all),
        "swap",
        [(value.shape[1:], value.dtype) for value in pair for _ in range(2)]
        + [((slots, rows), BF16), ((topk, rows), jnp.int32)],
        sent_last,
        expert_ids.T,
        *pair,
        far=range(2, 2 + len(pair)),
        unread=(0,),
        scratch=[pltpu.SemaphoreType.DMA((2 * len(pair),))],
        limit=8,
    )
    expert_mine = mine_and_theirs[::2]
    expert_got = [core_send(value) for value in mine_and_theirs[1::2]]

    away, keep, key_rows, value_rows, new_normer = call(
        functools.partial(cell_kernel, heads, size, chips, cols, ep_count - 1),
        "cell",
        [((rows, half), BF16), ((rows, half), F32)] + [((heads, size, rows), F32)] * 3,
        own,
        *sent,
        gates,
        matrix,
        normer,
        jnp.broadcast_to(head_gain[:, None], (heads * size, rows)),
        w_out,
        mine_and_theirs[0],
        unread=(ep_count + 5,),
        scratch=[pltpu.VMEM((span, rows), F32)],
        limit=20,
    )

    mix = keep + core_send(away).astype(F32)
    mix_parts = [mix[:, k * cols : (k + 1) * cols] for k in range(chips)]
    mix_sent = [mix_parts[k].astype(BF16) for k in range(1, chips)]
    mix_got = [chip_send(mix_sent[k - 1], k) for k in range(1, chips)]

    new_matrix, done = call(
        functools.partial(update_kernel, heads, size),
        "update",
        [((heads, size, size, rows), F32), ((8, 128), F32)],
        mix_sent[-1],
        matrix,
        key_rows,
        value_rows,
        gates,
        unread=(0,),
        far_out=(0,),
        scratch=[pltpu.VMEM((2, size, size, rows), F32), pltpu.SemaphoreType.DMA((2,))],
        limit=14,
    )

    (after_cols,) = call(
        after_kernel,
        "after",
        [((rows, cols), BF16)],
        done,
        own_resid,
        mix_parts[0],
        *mix_got,
        unread=(0,),
        limit=4,
    )
    after_parts = [after_cols] + [chip_send(after_cols, k) for k in range(1, chips)]
    after_other = core_send(jnp.concatenate(after_parts, axis=1))

    normed2, *buffers = call(
        functools.partial(dispatch_kernel, chips, cols, capacity),
        "dispatch",
        [((rows, width), BF16)] + [((capacity, width), BF16)] * ep_count,
        *after_parts,
        after_other,
        norm2_gain[None, :],
        picks,
        scratch=[pltpu.VMEM((rows, width), F32)],
        limit=10,
    )
    taken = [buffers[0]] + [ep_send(buffers[k], k) for k in others]

    combine_high, combine_low = call(
        functools.partial(route_kernel, per_group),
        "route",
        [((rows, slots), BF16)] * 2,
        normed2,
        group_router.T,
        expert_router.T,
        expert_ids.T,
        places,
    )

    terms = call(
        functools.partial(expert_kernel, ep_count),
        "experts",
        [((capacity, width), BF16)] * ep_count,
        *taken,
        *expert_mine,
        *expert_got,
        limit=14,
    )
    back = [terms[0]] + [ep_send(terms[k], k) for k in others]
    moe_away, moe_keep = call(
        functools.partial(combine_kernel, chips, cols, ep_count),
        "combine",
        [((rows, half), BF16), ((rows, half), F32)],
        *back,
        combine_high,
        combine_low,
    )
    moe = moe_keep + core_send(moe_away).astype(F32)
    moe_parts = [moe[:, k * cols : (k + 1) * cols] for k in range(chips)]
    moe_got = [chip_send(moe_parts[k].astype(BF16), k) for k in range(1, chips)]
    final = after_cols.astype(F32) + moe_parts[0]
    for value in moe_got:
        final = final + value.astype(F32)
    return (
        final.astype(BF16),
        new_matrix.transpose(3, 0, 1, 2),
        new_normer.transpose(2, 0, 1),
        new_max.T,
    )


def solution(mesh):
    in_specs = (
        P("ep", None),
        P(),
        P("ep", "tp"),
        P("ep", "tp"),
        P("ep", "tp"),
        P("ep", "tp"),
        P(),
        P(),
        P(),
        P("tp"),
        P("tp", None),
        P("ep", "tp", None, None),
        P("ep", "tp", None),
        P("ep", "tp"),
        P(),
        P(),
        P(),
        P("ep", None),
        P("ep", None, "tp"),
        P("ep", None, "tp"),
        P("ep", "tp", None),
    )
    out_specs = (P("ep", "tp"), P("ep", "tp", None, None), P("ep", "tp", None), P("ep", "tp"))
    return jax.shard_map(
        per_device, mesh=mesh, in_specs=in_specs, out_specs=out_specs, check_vma=False
    )
```

```python
import functools

import jax
import jax.numpy as jnp
from jax import lax
from jax.experimental import pallas as pl
from jax.experimental.pallas import tpu as pltpu
from jax.sharding import PartitionSpec as P


EPSILON = 1e-06
CORES = 2
VMEM = pltpu.MemorySpace.VMEM
F32, BF16 = jnp.float32, jnp.bfloat16


def ep_send(value, step):
    count = lax.axis_size("ep")
    return lax.ppermute(value, "ep", [(i, i ^ step) for i in range(count)])


def chip_send(value, step):
    count = lax.axis_size("tp")
    return lax.ppermute(value, "tp", [(i, i ^ (CORES * step)) for i in range(count)])


def core_send(value):
    count = lax.axis_size("tp")
    return lax.ppermute(value, "tp", [(i, i ^ 1) for i in range(count)])


def dot(lhs, rhs, lhs_dim, rhs_dim):
    return lax.dot_general(
        lhs, rhs, (((lhs_dim,), (rhs_dim,)), ((), ())), preferred_element_type=F32
    )


def call(kernel, outs, *args, far=(), unread=(), far_out=(), scratch=(), limit=8):
    args = [
        pltpu.with_memory_space_constraint(value, pltpu.MemorySpace.HBM) if i in far else value
        for i, value in enumerate(args)
    ]
    return pl.pallas_call(
        kernel,
        out_shape=[jax.ShapeDtypeStruct(shape, dtype) for shape, dtype in outs],
        in_specs=[
            pl.BlockSpec(memory_space=pl.ANY if i in far or i in unread else VMEM)
            for i in range(len(args))
        ],
        out_specs=[
            pl.BlockSpec(memory_space=pl.ANY if i in far_out else VMEM) for i in range(len(outs))
        ],
        scratch_shapes=list(scratch),
        compiler_params=pltpu.CompilerParams(vmem_limit_bytes=limit << 20),
    )(*args)


def block_cols(step, core, cols):
    chip = (lax.axis_index("tp") // CORES) ^ step
    return pl.ds(pl.multiple_of((chip * CORES + core) * cols, cols), cols)


def norm_kernel(steps, depth, cols, resid_ref, gain_ref, normed_ref, own_ref, *refs):
    block_refs, (rows_ref, row_ref, sems) = refs[:-3], refs[-3:]
    copies = [
        pltpu.make_async_copy(resid_ref, rows_ref, sems.at[0]),
        pltpu.make_async_copy(gain_ref, row_ref, sems.at[1]),
    ]
    for copy in copies:
        copy.start()
    for copy in copies:
        copy.wait()
    width = rows_ref.shape[1]
    wide = rows_ref[...].astype(F32)
    factor = lax.rsqrt(jnp.sum(wide * wide, axis=1, keepdims=True) / width + EPSILON)
    normed_ref[...] = (wide * factor * row_ref[...]).astype(BF16)
    for step, block_ref in zip(steps, block_refs):
        start = pl.multiple_of((lax.axis_index("ep") ^ step) * depth, depth)
        block_ref[...] = normed_ref[:, pl.ds(start, depth)]
    start = pl.multiple_of(lax.axis_index("tp") * cols, cols)
    own_ref[...] = rows_ref[:, pl.ds(start, cols)].astype(F32)


def gates_kernel(heads, count, normed_ref, *refs):
    gate_args, refs = refs[:4], refs[4:]
    sources, outs, refs = refs[:count], refs[count : 2 * count], refs[2 * count :]
    gates_ref, new_max_ref = refs[:2]
    igate_ref, fgate_ref, bias_ref, max_ref, both_ref, sems = refs[2:]
    targets = (igate_ref, fgate_ref, bias_ref, max_ref) + tuple(outs)
    copies = [
        pltpu.make_async_copy(source, target, sems.at[i])
        for i, (source, target) in enumerate(zip(tuple(gate_args) + tuple(sources), targets))
    ]
    for copy in copies:
        copy.start()
    for copy in copies[:4]:
        copy.wait()
    all_heads = igate_ref.shape[0]
    square = (all_heads, all_heads)
    diagonal = lax.broadcasted_iota(jnp.int32, square, 0) == lax.broadcasted_iota(
        jnp.int32, square, 1
    )
    bias = jnp.sum(jnp.where(diagonal, bias_ref[...], 0.0), axis=1, keepdims=True)
    both_ref[:all_heads] = dot(igate_ref[...], normed_ref[...], 1, 1)
    both_ref[all_heads:] = dot(fgate_ref[...], normed_ref[...], 1, 1) + bias
    start = lax.axis_index("tp") * heads
    in_gate = both_ref[pl.ds(start, heads)]
    forget = both_ref[pl.ds(all_heads + start, heads)]
    log_forget = jnp.minimum(forget, 0.0) - jnp.log1p(jnp.exp(-jnp.abs(forget)))
    running = log_forget + max_ref[...]
    new_max = jnp.maximum(running, in_gate)
    new_max_ref[...] = new_max
    gates_ref[:heads] = jnp.exp(running - new_max)
    gates_ref[heads:] = jnp.exp(in_gate - new_max)
    for copy in copies[4:]:
        copy.wait()


def stage_kernel(skip, count, chips, cols, *refs):
    w_ref, refs = refs[skip], refs[skip + 1 :]
    sources, outs = refs[:count], refs[count : 2 * count]
    keep_ref, away_ref, sems = refs[2 * count :]
    core = lax.axis_index("tp") % CORES
    pairs = list(zip(sources, outs))
    for out_ref, target in ((away_ref, 1 - core), (keep_ref, core)):
        for k in range(chips):
            at = pl.ds(k * cols, cols)
            pairs.append((w_ref.at[:, block_cols(k, target, cols)], out_ref.at[:, at]))
    copies = [
        pltpu.make_async_copy(source, target, sems.at[i])
        for i, (source, target) in enumerate(pairs)
    ]
    for copy in copies:
        copy.start()
    for copy in copies:
        copy.wait()


def swap_kernel(count, experts, after_ref, ids_ref, *refs):
    sources, outs = refs[:count], refs[count:-3]
    picks_ref, at_ref, sems = refs[-3:]
    core = lax.axis_index("tp") % CORES
    copies = []
    for i, source in enumerate(sources):
        for j, index in enumerate((core, 1 - core)):
            at = 2 * i + j
            copies.append(pltpu.make_async_copy(source.at[index], outs[at], sems.at[at]))
    for copy in copies:
        copy.start()
    topk, rows = ids_ref.shape
    slots = picks_ref.shape[0]
    local = sources[0].shape[0]
    capacity = slots // (experts // local)
    expert_iota = lax.broadcasted_iota(jnp.int32, (experts, rows), 0)
    hots = [(expert_iota == ids_ref[j : j + 1, :]).astype(F32) for j in range(topk)]
    before = lax.broadcasted_iota(jnp.int32, (rows, rows), 0) < lax.broadcasted_iota(
        jnp.int32, (rows, rows), 1
    )
    total = functools.reduce(lambda x, y: x + y, hots)
    earlier = dot(total.astype(BF16), before.astype(F32).astype(BF16), 1, 0)
    slot_iota = lax.broadcasted_iota(jnp.int32, (slots, rows), 0)
    picked = jnp.zeros((slots, rows), F32)
    for j in range(topk):
        ids = ids_ref[j : j + 1, :]
        slot = jnp.sum(earlier * hots[j], axis=0, keepdims=True).astype(jnp.int32)
        place = lax.shift_right_logical(ids, local.bit_length() - 1) ^ lax.axis_index("ep")
        at = jnp.where((ids & (local - 1)) == core, place * capacity + slot, -1)
        at_ref[j : j + 1, :] = at
        picked = picked + (slot_iota == at).astype(F32)
    picks_ref[...] = picked.astype(BF16)
    for copy in copies:
        copy.wait()


def update_kernel(heads, size, after_ref, matrix_ref, key_ref, value_ref, gates_ref, *refs):
    out_ref, done_ref, slots_ref, sems = refs
    copies = []
    for h in range(heads):
        slot = h % 2
        if h >= 2:
            copies[h - 2].wait()
        carried = gates_ref[h : h + 1, :]
        keys = key_ref[h] * gates_ref[heads + h : heads + h + 1, :]
        values = value_ref[h]
        for d in range(size):
            slots_ref[slot, d] = carried * matrix_ref[h, d] + keys[d : d + 1, :] * values
        copies.append(pltpu.make_async_copy(slots_ref.at[slot], out_ref.at[h], sems.at[slot]))
        copies[h].start()
    for copy in copies[-2:]:
        copy.wait()
    done_ref[...] = jnp.zeros_like(done_ref)


def project_kernel(x_ref, *refs):
    weights, out_ref = refs[:-1], refs[-1]
    cols = weights[0].shape[1]
    for i, w_ref in enumerate(weights):
        out_ref[:, i * cols : (i + 1) * cols] = jnp.dot(
            x_ref[...], w_ref[...], preferred_element_type=F32
        ).astype(out_ref.dtype)


def cell_kernel(heads, size, received, *refs):
    own_ref = refs[0]
    got_refs = refs[1 : 1 + received]
    gates_ref, matrix_ref, normer_ref, gain_ref = refs[1 + received : 5 + received]
    head_ref, key_ref, value_ref, norm_ref, turned_ref = refs[-5:]
    total = own_ref[...]
    for ref in got_refs:
        total = total + ref[...].astype(F32)
    turned_ref[...] = total.astype(BF16).astype(F32).T
    span = heads * size
    outs = []
    for h in range(heads):
        carried = gates_ref[h : h + 1, :]
        fresh = gates_ref[heads + h : heads + h + 1, :]
        scaled = turned_ref[h * size : (h + 1) * size, :] * size ** (-0.5)
        keys = turned_ref[span + h * size : span + (h + 1) * size, :]
        values = turned_ref[2 * span + h * size : 2 * span + (h + 1) * size, :]
        outgate = turned_ref[3 * span + h * size : 3 * span + (h + 1) * size, :]
        normer = normer_ref[h]
        readout = scaled[0:1, :] * matrix_ref[h, 0]
        for d in range(1, size):
            readout = readout + scaled[d : d + 1, :] * matrix_ref[h, d]
        score = jnp.sum(scaled * keys, axis=0, keepdims=True) * fresh
        numer = carried * readout + score * values
        denom = carried * jnp.sum(scaled * normer, axis=0, keepdims=True) + score
        cell = numer / jnp.maximum(jnp.abs(denom), 1.0)
        cell = cell * lax.rsqrt(jnp.mean(cell * cell, axis=0, keepdims=True) + EPSILON)
        outs.append(cell * jax.nn.sigmoid(outgate))
        key_ref[h] = keys
        value_ref[h] = values
        norm_ref[h] = carried * normer + fresh * keys
    head_ref[...] = (jnp.concatenate(outs, axis=0).T * gain_ref[...]).astype(BF16)


def mix_kernel(cols, own_ref, got_ref, w_own_ref, w_got_ref, keep_ref, *out_refs):
    own, got = own_ref[...], got_ref[...]
    for k, out_ref in enumerate((keep_ref,) + out_refs):
        at = slice(k * cols, (k + 1) * cols)
        value = jnp.dot(own, w_own_ref[:, at], preferred_element_type=F32)
        value = value + jnp.dot(got, w_got_ref[:, at], preferred_element_type=F32)
        out_ref[...] = value.astype(out_ref.dtype)


def after_kernel(done_ref, *refs):
    total = refs[0][...]
    for ref in refs[1:-1]:
        total = total + ref[...].astype(F32)
    refs[-1][...] = total.astype(BF16)


def route_kernel(per_group, normed_ref, group_ref, expert_ref, ids_ref, at_ref, *refs):
    high_ref, low_ref = refs
    rows, slots = high_ref.shape
    groups, experts = group_ref.shape[0], expert_ref.shape[0]
    group_exp = jnp.exp(dot(group_ref[...], normed_ref[...], 1, 1))
    group_prob = group_exp / jnp.sum(group_exp, axis=0, keepdims=True)
    logits = dot(expert_ref[...], normed_ref[...], 1, 1)
    expert_iota = lax.broadcasted_iota(jnp.int32, (experts, rows), 0)
    group_iota = lax.broadcasted_iota(jnp.int32, (groups, rows), 0)
    slot_iota = lax.broadcasted_iota(jnp.int32, (slots, rows), 0)
    chosen, shares = [], []
    for j in range(ids_ref.shape[0]):
        ids = ids_ref[j : j + 1, :]
        hot = expert_iota == ids
        chosen.append(jnp.exp(jnp.sum(jnp.where(hot, logits, 0.0), axis=0, keepdims=True)))
        first = group_iota * per_group
        hot = (first <= ids) & (ids < first + per_group)
        shares.append(jnp.sum(jnp.where(hot, group_prob, 0.0), axis=0, keepdims=True))
    total = functools.reduce(lambda x, y: x + y, chosen)
    combine = jnp.zeros((slots, rows), F32)
    for j, (value, share) in enumerate(zip(chosen, shares)):
        weight = share * value / total
        combine = combine + jnp.where(slot_iota == at_ref[j : j + 1, :], weight, 0.0)
    combine = combine.T
    high = combine.astype(BF16)
    high_ref[...] = high
    low_ref[...] = (combine - high.astype(F32)).astype(BF16)


def dispatch_kernel(chips, cols, capacity, *refs):
    own_refs = refs[:chips]
    other_ref, gain_ref, pick_ref = refs[chips : chips + 3]
    normed_ref, out_refs, full_ref = refs[chips + 3], refs[chips + 4 : -1], refs[-1]
    core = lax.axis_index("tp") % CORES
    for k in range(chips):
        full_ref[:, block_cols(k, core, cols)] = own_refs[k][...].astype(F32)
        full_ref[:, block_cols(k, 1 - core, cols)] = other_ref[
            :, k * cols : (k + 1) * cols
        ].astype(F32)
    full = full_ref[...]
    factor = lax.rsqrt(jnp.sum(full * full, axis=1, keepdims=True) / full.shape[1] + EPSILON)
    normed = (full * factor * gain_ref[...]).astype(BF16)
    normed_ref[...] = normed
    picked = jnp.dot(pick_ref[...], normed, preferred_element_type=F32)
    for k, out_ref in enumerate(out_refs):
        out_ref[...] = picked[k * capacity : (k + 1) * capacity].astype(BF16)


def expert_kernel(x_ref, *refs):
    weights, out_ref = refs[:6], refs[6]
    x = x_ref[...]
    result = None
    for gate_ref, up_ref, down_ref in (weights[:3], weights[3:]):
        gate = jnp.dot(x, gate_ref[...], preferred_element_type=F32)
        up = jnp.dot(x, up_ref[...], preferred_element_type=F32)
        units = (jax.nn.silu(gate) * up).astype(BF16)
        part = jnp.dot(units, down_ref[...], preferred_element_type=F32)
        result = part if result is None else result + part
    out_ref[...] = result.astype(BF16)


def combine_kernel(chips, cols, blocks, *refs):
    y_refs = refs[:blocks]
    high_ref, low_ref, away_ref, keep_ref = refs[blocks:]
    core = lax.axis_index("tp") % CORES
    for k in range(chips):
        at = slice(k * cols, (k + 1) * cols)
        for target, out_ref in ((1 - core, away_ref), (core, keep_ref)):
            ds = block_cols(k, target, cols)
            y = jnp.concatenate([ref[:, ds] for ref in y_refs], axis=0)
            value = jnp.dot(high_ref[...], y, preferred_element_type=F32)
            value = value + jnp.dot(low_ref[...], y, preferred_element_type=F32)
            out_ref[:, at] = value.astype(out_ref.dtype)


def per_device(
    resid,
    norm1_gain,
    w_query,
    w_key,
    w_value,
    w_outgate,
    w_igate,
    w_fgate,
    forget_bias,
    head_gain,
    w_out,
    state_matrix,
    state_norm,
    state_max,
    norm2_gain,
    group_router,
    expert_router,
    expert_ids,
    exp_gate,
    exp_up,
    exp_down,
):
    rows, width = resid.shape
    heads, size = state_matrix.shape[1], state_matrix.shape[2]
    ep_count, tp_count = lax.axis_size("ep"), lax.axis_size("tp")
    chips = tp_count // CORES
    cols = width // tp_count
    depth = w_query.shape[0]
    experts_all, groups = expert_router.shape[1], group_router.shape[1]
    per_group = experts_all // groups
    topk = expert_ids.shape[1]
    local_experts, _, _ = exp_gate.shape
    assert local_experts == CORES
    capacity = max(2, 3 * rows * topk // (2 * experts_all))
    half = chips * cols
    others = range(1, ep_count)

    normed, own_resid, *blocks = call(
        functools.partial(norm_kernel, range(ep_count), depth, cols),
        [((rows, width), BF16), ((rows, cols), F32)] + [((rows, depth), BF16)] * ep_count,
        resid,
        norm1_gain[None, :],
        far=(0, 1),
        scratch=[
            pltpu.VMEM((rows, width), BF16),
            pltpu.VMEM((1, width), F32),
            pltpu.SemaphoreType.DMA((2,)),
        ],
    )
    arrived = [ep_send(blocks[k], k) for k in others]
    matrix = state_matrix.transpose(1, 2, 3, 0)
    normer = state_norm.transpose(1, 2, 0)
    weights = (w_query, w_key, w_value, w_outgate)
    all_heads = w_igate.shape[1]
    *weights, gates, new_max = call(
        functools.partial(gates_kernel, heads, len(weights)),
        [(value.shape, value.dtype) for value in weights]
        + [((2 * heads, rows), F32), ((heads, rows), F32)],
        normed,
        w_igate.T,
        w_fgate.T,
        forget_bias[None, :],
        state_max.T,
        *weights,
        far=range(1, 5 + len(weights)),
        scratch=[
            pltpu.VMEM((all_heads, width), BF16),
            pltpu.VMEM((all_heads, width), BF16),
            pltpu.VMEM((1, all_heads), F32),
            pltpu.VMEM((heads, rows), F32),
            pltpu.VMEM((2 * all_heads, rows), F32),
            pltpu.SemaphoreType.DMA((4 + len(weights),)),
        ],
    )
    span = 4 * heads * size
    (own,) = call(project_kernel, [((rows, span), F32)], blocks[0], *weights)
    parts, sent = [], []
    for k in others:
        (part,) = call(project_kernel, [((rows, span), BF16)], arrived[k - 1], *weights)
        parts.append(part)
        sent.append(ep_send(part, k))

    stage_outs = [(value.shape, value.dtype) for value in (matrix, normer)]
    stage_outs += [((heads * size, half), BF16)] * 2
    matrix, normer, w_own, w_sent = call(
        functools.partial(stage_kernel, len(parts), 2, chips, cols),
        stage_outs,
        *parts,
        w_out,
        matrix,
        normer,
        far=range(len(parts), len(parts) + 3),
        unread=range(len(parts)),
        scratch=[pltpu.SemaphoreType.DMA((2 + 2 * chips,))],
        limit=16,
    )
    w_got = core_send(w_sent)

    pair = (exp_gate, exp_up, exp_down)
    slots = ep_count * capacity
    *mine_and_theirs, picks, places = call(
        functools.partial(swap_kernel, len(pair), experts_all),
        [(value.shape[1:], value.dtype) for value in pair for _ in range(2)]
        + [((slots, rows), BF16), ((topk, rows), jnp.int32)],
        w_sent,
        expert_ids.T,
        *pair,
        far=range(2, 2 + len(pair)),
        unread=(0,),
        scratch=[pltpu.SemaphoreType.DMA((2 * len(pair),))],
        limit=8,
    )
    expert_mine = mine_and_theirs[::2]
    expert_got = [core_send(value) for value in mine_and_theirs[1::2]]

    head_out, key_rows, value_rows, new_normer = call(
        functools.partial(cell_kernel, heads, size, ep_count - 1),
        [((rows, heads * size), BF16)] + [((heads, size, rows), F32)] * 3,
        own,
        *sent,
        gates,
        matrix,
        normer,
        head_gain[None, :],
        mine_and_theirs[0],
        w_got,
        unread=(ep_count + 4, ep_count + 5),
        scratch=[pltpu.VMEM((span, rows), F32)],
        limit=20,
    )

    mix_own, *mix_sent = call(
        functools.partial(mix_kernel, cols),
        [((rows, cols), F32)] + [((rows, cols), BF16)] * (chips - 1),
        head_out,
        core_send(head_out),
        w_own,
        w_got,
    )
    mix_got = [chip_send(mix_sent[k - 1], k) for k in range(1, chips)]

    new_matrix, done = call(
        functools.partial(update_kernel, heads, size),
        [((heads, size, size, rows), F32), ((8, 128), F32)],
        mix_sent[-1],
        matrix,
        key_rows,
        value_rows,
        gates,
        unread=(0,),
        far_out=(0,),
        scratch=[pltpu.VMEM((2, size, size, rows), F32), pltpu.SemaphoreType.DMA((2,))],
        limit=14,
    )

    (after_cols,) = call(
        after_kernel,
        [((rows, cols), BF16)],
        done,
        own_resid,
        mix_own,
        *mix_got,
        unread=(0,),
        limit=4,
    )
    after_parts = [after_cols] + [chip_send(after_cols, k) for k in range(1, chips)]
    after_other = core_send(jnp.concatenate(after_parts, axis=1))

    normed2, *buffers = call(
        functools.partial(dispatch_kernel, chips, cols, capacity),
        [((rows, width), BF16)] + [((capacity, width), BF16)] * ep_count,
        *after_parts,
        after_other,
        norm2_gain[None, :],
        picks,
        scratch=[pltpu.VMEM((rows, width), F32)],
        limit=10,
    )
    taken = [buffers[0]] + [ep_send(buffers[k], k) for k in others]

    combine_high, combine_low = call(
        functools.partial(route_kernel, per_group),
        [((rows, slots), BF16)] * 2,
        normed2,
        group_router.T,
        expert_router.T,
        expert_ids.T,
        places,
    )

    terms = []
    for k in range(ep_count):
        (part,) = call(
            expert_kernel,
            [((capacity, width), BF16)],
            taken[k],
            *expert_mine,
            *expert_got,
            limit=12,
        )
        terms.append(part)
    back = [terms[0]] + [ep_send(terms[k], k) for k in others]
    moe_away, moe_keep = call(
        functools.partial(combine_kernel, chips, cols, ep_count),
        [((rows, half), BF16), ((rows, half), F32)],
        *back,
        combine_high,
        combine_low,
    )
    moe = moe_keep + core_send(moe_away).astype(F32)
    moe_parts = [moe[:, k * cols : (k + 1) * cols] for k in range(chips)]
    moe_got = [chip_send(moe_parts[k].astype(BF16), k) for k in range(1, chips)]
    final = after_cols.astype(F32) + moe_parts[0]
    for value in moe_got:
        final = final + value.astype(F32)
    return (
        final.astype(BF16),
        new_matrix.transpose(3, 0, 1, 2),
        new_normer.transpose(2, 0, 1),
        new_max.T,
    )


def solution(mesh):
    in_specs = (
        P("ep", None),
        P(),
        P("ep", "tp"),
        P("ep", "tp"),
        P("ep", "tp"),
        P("ep", "tp"),
        P(),
        P(),
        P(),
        P("tp"),
        P("tp", None),
        P("ep", "tp", None, None),
        P("ep", "tp", None),
        P("ep", "tp"),
        P(),
        P(),
        P(),
        P("ep", None),
        P("ep", None, "tp"),
        P("ep", None, "tp"),
        P("ep", "tp", None),
    )
    out_specs = (P("ep", "tp"), P("ep", "tp", None, None), P("ep", "tp", None), P("ep", "tp"))
    return jax.shard_map(
        per_device, mesh=mesh, in_specs=in_specs, out_specs=out_specs, check_vma=False
    )
```

```python
import functools

import jax
import jax.numpy as jnp
from jax import lax
from jax.experimental import pallas as pl
from jax.experimental.pallas import tpu as pltpu
from jax.sharding import PartitionSpec as P


EPSILON = 1e-06
CORES = 2
VMEM = pltpu.MemorySpace.VMEM
F32, BF16 = jnp.float32, jnp.bfloat16


def ep_send(value, step):
    count = lax.axis_size("ep")
    return lax.ppermute(value, "ep", [(i, i ^ step) for i in range(count)])


def chip_send(value, step):
    count = lax.axis_size("tp")
    return lax.ppermute(value, "tp", [(i, i ^ (CORES * step)) for i in range(count)])


def core_send(value):
    count = lax.axis_size("tp")
    return lax.ppermute(value, "tp", [(i, i ^ 1) for i in range(count)])


def dot(lhs, rhs, lhs_dim, rhs_dim):
    return lax.dot_general(
        lhs, rhs, (((lhs_dim,), (rhs_dim,)), ((), ())), preferred_element_type=F32
    )


def call(kernel, outs, *args, far=(), unread=(), far_out=(), scratch=(), limit=8):
    args = [
        pltpu.with_memory_space_constraint(value, pltpu.MemorySpace.HBM) if i in far else value
        for i, value in enumerate(args)
    ]
    return pl.pallas_call(
        kernel,
        out_shape=[jax.ShapeDtypeStruct(shape, dtype) for shape, dtype in outs],
        in_specs=[
            pl.BlockSpec(memory_space=pl.ANY if i in far or i in unread else VMEM)
            for i in range(len(args))
        ],
        out_specs=[
            pl.BlockSpec(memory_space=pl.ANY if i in far_out else VMEM) for i in range(len(outs))
        ],
        scratch_shapes=list(scratch),
        compiler_params=pltpu.CompilerParams(vmem_limit_bytes=limit << 20),
    )(*args)


def block_cols(step, core, cols):
    chip = (lax.axis_index("tp") // CORES) ^ step
    return pl.ds(pl.multiple_of((chip * CORES + core) * cols, cols), cols)


def split_kernel(depth, resid_ref, *refs):
    out_refs, sems = refs[:-1], refs[-1]
    copies = []
    for step, out_ref in enumerate(out_refs):
        start = pl.multiple_of((lax.axis_index("ep") ^ step) * depth, depth)
        copies.append(
            pltpu.make_async_copy(resid_ref.at[:, pl.ds(start, depth)], out_ref, sems.at[step])
        )
    for copy in copies:
        copy.start()
    for copy in copies:
        copy.wait()


def load_kernel(count, depth, gain_ref, *refs):
    sources, outs, sems = refs[:count], refs[count : 2 * count], refs[-1]
    start = pl.multiple_of(lax.axis_index("ep") * depth, depth)
    pairs = [(gain_ref.at[:, pl.ds(start, depth)], refs[2 * count])] + list(zip(sources, outs))
    copies = [
        pltpu.make_async_copy(source, target, sems.at[i])
        for i, (source, target) in enumerate(pairs)
    ]
    for copy in copies:
        copy.start()
    for copy in copies:
        copy.wait()


def gates_step(heads, cols, targets, outs, both_ref):
    igate_ref, fgate_ref, bias_ref, max_ref, rows_ref, row_ref = targets
    gates_ref, new_max_ref, factor_ref, own_ref = outs
    wide = rows_ref[...].astype(F32)
    factor = lax.rsqrt(jnp.mean(wide * wide, axis=1, keepdims=True) + EPSILON)
    normed = (wide * factor * row_ref[...]).astype(BF16)
    factor_ref[...] = jnp.broadcast_to(factor, factor_ref.shape)
    start = pl.multiple_of(lax.axis_index("tp") * cols, cols)
    own_ref[...] = rows_ref[:, pl.ds(start, cols)].astype(F32)
    all_heads = igate_ref.shape[0]
    square = (all_heads, all_heads)
    diagonal = lax.broadcasted_iota(jnp.int32, square, 0) == lax.broadcasted_iota(
        jnp.int32, square, 1
    )
    bias = jnp.sum(jnp.where(diagonal, bias_ref[...], 0.0), axis=1, keepdims=True)
    both_ref[:all_heads] = dot(igate_ref[...], normed, 1, 1)
    both_ref[all_heads:] = dot(fgate_ref[...], normed, 1, 1) + bias
    start = lax.axis_index("tp") * heads
    in_gate = both_ref[pl.ds(start, heads)]
    forget = both_ref[pl.ds(all_heads + start, heads)]
    log_forget = jnp.minimum(forget, 0.0) - jnp.log1p(jnp.exp(-jnp.abs(forget)))
    running = log_forget + max_ref[...]
    new_max = jnp.maximum(running, in_gate)
    new_max_ref[...] = new_max
    gates_ref[:heads] = jnp.exp(running - new_max)
    gates_ref[heads:] = jnp.exp(in_gate - new_max)


def slots_step(experts, local, ids_ref, picks_ref, at_ref):
    core = lax.axis_index("tp") % CORES
    topk, rows = ids_ref.shape
    slots = picks_ref.shape[0]
    capacity = slots // (experts // local)
    expert_iota = lax.broadcasted_iota(jnp.int32, (experts, rows), 0)
    hots = [(expert_iota == ids_ref[j : j + 1, :]).astype(F32) for j in range(topk)]
    before = lax.broadcasted_iota(jnp.int32, (rows, rows), 0) < lax.broadcasted_iota(
        jnp.int32, (rows, rows), 1
    )
    total = functools.reduce(lambda x, y: x + y, hots)
    earlier = dot(total.astype(BF16), before.astype(F32).astype(BF16), 1, 0)
    slot_iota = lax.broadcasted_iota(jnp.int32, (slots, rows), 0)
    picked = jnp.zeros((slots, rows), F32)
    for j in range(topk):
        ids = ids_ref[j : j + 1, :]
        slot = jnp.sum(earlier * hots[j], axis=0, keepdims=True).astype(jnp.int32)
        place = lax.shift_right_logical(ids, local.bit_length() - 1) ^ lax.axis_index("ep")
        at = jnp.where((ids & (local - 1)) == core, place * capacity + slot, -1)
        at_ref[j : j + 1, :] = at
        picked = picked + (slot_iota == at).astype(F32)
    picks_ref[...] = picked.astype(BF16)


def stage_kernel(skip, heads, chips, cols, experts, *refs):
    ids_ref, refs = refs[skip], refs[skip + 1 :]
    gate_sources, (w_ref, matrix_ref, normer_ref), pair = refs[:6], refs[6:9], refs[9:12]
    outs, scratch = refs[12:28], refs[28:]
    targets, both_ref, sems = scratch[:6], scratch[6], scratch[7]
    core = lax.axis_index("tp") % CORES
    away_ref, keep_ref, matrix_out, normer_out = outs[:4]
    pairs = list(zip(gate_sources, targets))
    for out_ref, target in ((away_ref, 1 - core), (keep_ref, core)):
        for k in range(chips):
            at = pl.ds(k * cols, cols)
            pairs.append((w_ref.at[:, block_cols(k, target, cols)], out_ref.at[:, at]))
    for i, source in enumerate(pair):
        pairs.append((source.at[1 - core], outs[4 + i]))
        pairs.append((source.at[core], outs[7 + i]))
    pairs += [(normer_ref, normer_out), (matrix_ref, matrix_out)]
    copies = [
        pltpu.make_async_copy(source, target, sems.at[i])
        for i, (source, target) in enumerate(pairs)
    ]
    for copy in copies:
        copy.start()
    slots_step(experts, pair[0].shape[0], ids_ref, outs[14], outs[15])
    for copy in copies[:6]:
        copy.wait()
    gates_step(heads, cols, targets, outs[10:14], both_ref)
    for copy in copies[6:]:
        copy.wait()


def update_kernel(heads, size, after_ref, matrix_ref, key_ref, value_ref, gates_ref, *refs):
    out_ref, done_ref, slots_ref, sems = refs
    copies = []
    for h in range(heads):
        slot = h % 2
        if h >= 2:
            copies[h - 2].wait()
        carried = gates_ref[h : h + 1, :]
        keys = key_ref[h] * gates_ref[heads + h : heads + h + 1, :]
        values = value_ref[h]
        for d in range(size):
            slots_ref[slot, d] = carried * matrix_ref[h, d] + keys[d : d + 1, :] * values
        copies.append(pltpu.make_async_copy(slots_ref.at[slot], out_ref.at[h], sems.at[slot]))
        copies[h].start()
    for copy in copies[-2:]:
        copy.wait()
    done_ref[...] = jnp.zeros_like(done_ref)


def project_kernel(x_ref, gain_ref, *refs):
    weights, out_ref = refs[:-1], refs[-1]
    cols = weights[0].shape[1]
    x = (x_ref[...].astype(F32) * gain_ref[...]).astype(BF16)
    for i, w_ref in enumerate(weights):
        out_ref[:, i * cols : (i + 1) * cols] = jnp.dot(
            x, w_ref[...], preferred_element_type=F32
        ).astype(out_ref.dtype)


def cell_kernel(heads, size, received, *refs):
    own_ref = refs[0]
    got_refs = refs[1 : 1 + received]
    gates_ref, matrix_ref, normer_ref, gain_ref, factor_ref = refs[1 + received : 6 + received]
    head_ref, key_ref, value_ref, norm_ref, turned_ref = refs[-5:]
    total = own_ref[...]
    for ref in got_refs:
        total = total + ref[...].astype(F32)
    total = total * factor_ref[:, :1]
    turned_ref[...] = total.astype(BF16).astype(F32).T
    span = heads * size
    outs = []
    for h in range(heads):
        carried = gates_ref[h : h + 1, :]
        fresh = gates_ref[heads + h : heads + h + 1, :]
        scaled = turned_ref[h * size : (h + 1) * size, :] * size ** (-0.5)
        keys = turned_ref[span + h * size : span + (h + 1) * size, :]
        values = turned_ref[2 * span + h * size : 2 * span + (h + 1) * size, :]
        outgate = turned_ref[3 * span + h * size : 3 * span + (h + 1) * size, :]
        normer = normer_ref[h]
        readout = scaled[0:1, :] * matrix_ref[h, 0]
        for d in range(1, size):
            readout = readout + scaled[d : d + 1, :] * matrix_ref[h, d]
        score = jnp.sum(scaled * keys, axis=0, keepdims=True) * fresh
        numer = carried * readout + score * values
        denom = carried * jnp.sum(scaled * normer, axis=0, keepdims=True) + score
        cell = numer / jnp.maximum(jnp.abs(denom), 1.0)
        cell = cell * lax.rsqrt(jnp.mean(cell * cell, axis=0, keepdims=True) + EPSILON)
        outs.append(cell * jax.nn.sigmoid(outgate))
        key_ref[h] = keys
        value_ref[h] = values
        norm_ref[h] = carried * normer + fresh * keys
    head_ref[...] = (jnp.concatenate(outs, axis=0).T * gain_ref[...]).astype(BF16)


def mix_kernel(cols, own_ref, got_ref, w_own_ref, w_got_ref, keep_ref, *out_refs):
    own, got = own_ref[...], got_ref[...]
    for k, out_ref in enumerate((keep_ref,) + out_refs):
        at = slice(k * cols, (k + 1) * cols)
        value = jnp.dot(own, w_own_ref[:, at], preferred_element_type=F32)
        value = value + jnp.dot(got, w_got_ref[:, at], preferred_element_type=F32)
        out_ref[...] = value.astype(out_ref.dtype)


def final_kernel(*refs):
    total = refs[0][...].astype(F32)
    for ref in refs[1:-1]:
        total = total + ref[...].astype(F32)
    refs[-1][...] = total.astype(BF16)


def after_kernel(done_ref, *refs):
    final_kernel(*refs)


def route_kernel(per_group, normed_ref, group_ref, expert_ref, ids_ref, at_ref, *refs):
    high_ref, low_ref = refs
    rows, slots = high_ref.shape
    groups, experts = group_ref.shape[0], expert_ref.shape[0]
    group_exp = jnp.exp(dot(group_ref[...], normed_ref[...], 1, 1))
    group_prob = group_exp / jnp.sum(group_exp, axis=0, keepdims=True)
    logits = dot(expert_ref[...], normed_ref[...], 1, 1)
    expert_iota = lax.broadcasted_iota(jnp.int32, (experts, rows), 0)
    group_iota = lax.broadcasted_iota(jnp.int32, (groups, rows), 0)
    slot_iota = lax.broadcasted_iota(jnp.int32, (slots, rows), 0)
    chosen, shares = [], []
    for j in range(ids_ref.shape[0]):
        ids = ids_ref[j : j + 1, :]
        hot = expert_iota == ids
        chosen.append(jnp.exp(jnp.sum(jnp.where(hot, logits, 0.0), axis=0, keepdims=True)))
        first = group_iota * per_group
        hot = (first <= ids) & (ids < first + per_group)
        shares.append(jnp.sum(jnp.where(hot, group_prob, 0.0), axis=0, keepdims=True))
    total = functools.reduce(lambda x, y: x + y, chosen)
    combine = jnp.zeros((slots, rows), F32)
    for j, (value, share) in enumerate(zip(chosen, shares)):
        weight = share * value / total
        combine = combine + jnp.where(slot_iota == at_ref[j : j + 1, :], weight, 0.0)
    combine = combine.T
    high = combine.astype(BF16)
    high_ref[...] = high
    low_ref[...] = (combine - high.astype(F32)).astype(BF16)


def dispatch_kernel(chips, cols, capacity, *refs):
    own_refs = refs[:chips]
    other_refs, refs = refs[chips : 2 * chips], refs[2 * chips :]
    gain_ref, pick_ref, normed_ref = refs[:3]
    out_refs, full_ref = refs[3:-1], refs[-1]
    core = lax.axis_index("tp") % CORES
    for k in range(chips):
        full_ref[:, block_cols(k, core, cols)] = own_refs[k][...].astype(F32)
        full_ref[:, block_cols(k, 1 - core, cols)] = other_refs[k][...].astype(F32)
    full = full_ref[...]
    factor = lax.rsqrt(jnp.sum(full * full, axis=1, keepdims=True) / full.shape[1] + EPSILON)
    normed = (full * factor * gain_ref[...]).astype(BF16)
    normed_ref[...] = normed
    picked = jnp.dot(pick_ref[...], normed, preferred_element_type=F32)
    for k, out_ref in enumerate(out_refs):
        out_ref[...] = picked[k * capacity : (k + 1) * capacity].astype(BF16)


def expert_kernel(x_ref, *refs):
    weights, out_ref = refs[:6], refs[6]
    x = x_ref[...]
    result = None
    for gate_ref, up_ref, down_ref in (weights[:3], weights[3:]):
        gate = jnp.dot(x, gate_ref[...], preferred_element_type=F32)
        up = jnp.dot(x, up_ref[...], preferred_element_type=F32)
        units = (jax.nn.silu(gate) * up).astype(BF16)
        part = jnp.dot(units, down_ref[...], preferred_element_type=F32)
        result = part if result is None else result + part
    out_ref[...] = result.astype(BF16)


def combine_kernel(chips, cols, blocks, *refs):
    y_refs = refs[:blocks]
    high_ref, low_ref, away_ref, keep_ref = refs[blocks:]
    core = lax.axis_index("tp") % CORES
    for k in range(chips):
        at = slice(k * cols, (k + 1) * cols)
        for target, out_ref in ((1 - core, away_ref), (core, keep_ref)):
            ds = block_cols(k, target, cols)
            y = jnp.concatenate([ref[:, ds] for ref in y_refs], axis=0)
            value = jnp.dot(high_ref[...], y, preferred_element_type=F32)
            value = value + jnp.dot(low_ref[...], y, preferred_element_type=F32)
            out_ref[:, at] = value.astype(out_ref.dtype)


def per_device(
    resid,
    norm1_gain,
    w_query,
    w_key,
    w_value,
    w_outgate,
    w_igate,
    w_fgate,
    forget_bias,
    head_gain,
    w_out,
    state_matrix,
    state_norm,
    state_max,
    norm2_gain,
    group_router,
    expert_router,
    expert_ids,
    exp_gate,
    exp_up,
    exp_down,
):
    rows, width = resid.shape
    heads, size = state_matrix.shape[1], state_matrix.shape[2]
    ep_count, tp_count = lax.axis_size("ep"), lax.axis_size("tp")
    chips = tp_count // CORES
    cols = width // tp_count
    depth = w_query.shape[0]
    experts_all, groups = expert_router.shape[1], group_router.shape[1]
    per_group = experts_all // groups
    topk = expert_ids.shape[1]
    local_experts, _, _ = exp_gate.shape
    assert local_experts == CORES
    capacity = max(2, 3 * rows * topk // (2 * experts_all))
    half = chips * cols
    others = range(1, ep_count)

    blocks = call(
        functools.partial(split_kernel, depth),
        [((rows, depth), BF16)] * ep_count,
        resid,
        far=(0,),
        scratch=[pltpu.SemaphoreType.DMA((ep_count,))],
    )
    arrived = [ep_send(blocks[k], k) for k in others]
    matrix = state_matrix.transpose(1, 2, 3, 0)
    normer = state_norm.transpose(1, 2, 0)
    weights = (w_query, w_key, w_value, w_outgate)
    *weights, gain = call(
        functools.partial(load_kernel, len(weights), depth),
        [(value.shape, value.dtype) for value in weights] + [((1, depth), F32)],
        norm1_gain[None, :],
        *weights,
        far=range(1 + len(weights)),
        scratch=[pltpu.SemaphoreType.DMA((1 + len(weights),))],
    )
    weights = [gain] + weights
    span = 4 * heads * size
    (own,) = call(project_kernel, [((rows, span), F32)], blocks[0], *weights)
    parts, sent = [], []
    for k in others:
        (part,) = call(project_kernel, [((rows, span), BF16)], arrived[k - 1], *weights)
        parts.append(part)
        sent.append(ep_send(part, k))

    all_heads = w_igate.shape[1]
    slots = ep_count * capacity
    pair = (exp_gate, exp_up, exp_down)
    expert_outs = [(value.shape[1:], value.dtype) for value in pair]
    w_sent, w_own, matrix, normer, *staged = call(
        functools.partial(stage_kernel, len(parts), heads, chips, cols, experts_all),
        [((heads * size, half), BF16)] * 2
        + [(matrix.shape, F32), (normer.shape, F32)]
        + expert_outs * 2
        + [((2 * heads, rows), F32), ((heads, rows), F32)]
        + [((rows, 128), F32), ((rows, cols), F32)]
        + [((slots, rows), BF16), ((topk, rows), jnp.int32)],
        *parts,
        expert_ids.T,
        w_igate.T,
        w_fgate.T,
        forget_bias[None, :],
        state_max.T,
        resid,
        norm1_gain[None, :],
        w_out,
        matrix,
        normer,
        *pair,
        far=range(len(parts) + 1, len(parts) + 13),
        unread=range(len(parts)),
        scratch=[
            pltpu.VMEM((all_heads, width), BF16),
            pltpu.VMEM((all_heads, width), BF16),
            pltpu.VMEM((1, all_heads), F32),
            pltpu.VMEM((heads, rows), F32),
            pltpu.VMEM((rows, width), BF16),
            pltpu.VMEM((1, width), F32),
            pltpu.VMEM((2 * all_heads, rows), F32),
            pltpu.SemaphoreType.DMA((14 + 2 * chips,)),
        ],
        limit=24,
    )
    expert_sent, expert_mine = staged[:3], staged[3:6]
    gates, new_max, factor, own_resid, picks, places = staged[6:]
    w_got = core_send(w_sent)
    expert_got = [core_send(value) for value in expert_sent]

    head_out, key_rows, value_rows, new_normer = call(
        functools.partial(cell_kernel, heads, size, ep_count - 1),
        [((rows, heads * size), BF16)] + [((heads, size, rows), F32)] * 3,
        own,
        *sent,
        gates,
        matrix,
        normer,
        head_gain[None, :],
        factor,
        w_got,
        unread=(ep_count + 5,),
        scratch=[pltpu.VMEM((span, rows), F32)],
        limit=20,
    )

    mix_own, *mix_sent = call(
        functools.partial(mix_kernel, cols),
        [((rows, cols), F32)] + [((rows, cols), BF16)] * (chips - 1),
        head_out,
        core_send(head_out),
        w_own,
        w_got,
    )
    mix_got = [chip_send(mix_sent[k - 1], k) for k in range(1, chips)]

    new_matrix, done = call(
        functools.partial(update_kernel, heads, size),
        [((heads, size, size, rows), F32), ((8, 128), F32)],
        mix_sent[-1],
        matrix,
        key_rows,
        value_rows,
        gates,
        unread=(0,),
        far_out=(0,),
        scratch=[pltpu.VMEM((2, size, size, rows), F32), pltpu.SemaphoreType.DMA((2,))],
        limit=14,
    )

    (after_cols,) = call(
        after_kernel,
        [((rows, cols), BF16)],
        done,
        own_resid,
        mix_own,
        *mix_got,
        unread=(0,),
        limit=4,
    )
    after_parts = [after_cols] + [chip_send(after_cols, k) for k in range(1, chips)]
    after_others = [core_send(part) for part in after_parts]

    normed2, *buffers = call(
        functools.partial(dispatch_kernel, chips, cols, capacity),
        [((rows, width), BF16)] + [((capacity, width), BF16)] * ep_count,
        *after_parts,
        *after_others,
        norm2_gain[None, :],
        picks,
        scratch=[pltpu.VMEM((rows, width), F32)],
        limit=10,
    )
    taken = [buffers[0]] + [ep_send(buffers[k], k) for k in others]

    combine_high, combine_low = call(
        functools.partial(route_kernel, per_group),
        [((rows, slots), BF16)] * 2,
        normed2,
        group_router.T,
        expert_router.T,
        expert_ids.T,
        places,
    )

    terms = []
    for k in range(ep_count):
        (part,) = call(
            expert_kernel,
            [((capacity, width), BF16)],
            taken[k],
            *expert_mine,
            *expert_got,
            limit=12,
        )
        terms.append(part)
    back = [terms[0]] + [ep_send(terms[k], k) for k in others]
    moe_away, moe_keep = call(
        functools.partial(combine_kernel, chips, cols, ep_count),
        [((rows, half), BF16), ((rows, half), F32)],
        *back,
        combine_high,
        combine_low,
    )
    moe = moe_keep + core_send(moe_away).astype(F32)
    moe_parts = [moe[:, k * cols : (k + 1) * cols] for k in range(chips)]
    moe_got = [chip_send(moe_parts[k].astype(BF16), k) for k in range(1, chips)]
    (mixed,) = call(
        final_kernel, [((rows, cols), BF16)], after_cols, moe_parts[0], *moe_got, limit=4
    )
    return (
        mixed,
        new_matrix.transpose(3, 0, 1, 2),
        new_normer.transpose(2, 0, 1),
        new_max.T,
    )


def solution(mesh):
    in_specs = (
        P("ep", None),
        P(),
        P("ep", "tp"),
        P("ep", "tp"),
        P("ep", "tp"),
        P("ep", "tp"),
        P(),
        P(),
        P(),
        P("tp"),
        P("tp", None),
        P("ep", "tp", None, None),
        P("ep", "tp", None),
        P("ep", "tp"),
        P(),
        P(),
        P(),
        P("ep", None),
        P("ep", None, "tp"),
        P("ep", None, "tp"),
        P("ep", "tp", None),
    )
    out_specs = (P("ep", "tp"), P("ep", "tp", None, None), P("ep", "tp", None), P("ep", "tp"))
    return jax.shard_map(
        per_device, mesh=mesh, in_specs=in_specs, out_specs=out_specs, check_vma=False
    )
```

```python
import functools

import jax
import jax.numpy as jnp
from jax import lax
from jax.experimental import pallas as pl
from jax.experimental.pallas import tpu as pltpu
from jax.sharding import PartitionSpec as P


EPSILON = 1e-06
CORES = 2
VMEM = pltpu.MemorySpace.VMEM
F32, BF16 = jnp.float32, jnp.bfloat16


def ep_send(value, step):
    count = lax.axis_size("ep")
    return lax.ppermute(value, "ep", [(i, i ^ step) for i in range(count)])


def chip_send(value, step):
    count = lax.axis_size("tp")
    return lax.ppermute(value, "tp", [(i, i ^ (CORES * step)) for i in range(count)])


def core_send(value):
    count = lax.axis_size("tp")
    return lax.ppermute(value, "tp", [(i, i ^ 1) for i in range(count)])


def dot(lhs, rhs, lhs_dim, rhs_dim):
    return lax.dot_general(
        lhs, rhs, (((lhs_dim,), (rhs_dim,)), ((), ())), preferred_element_type=F32
    )


def call(kernel, outs, *args, far=(), unread=(), far_out=(), scratch=(), limit=8):
    args = [
        pltpu.with_memory_space_constraint(value, pltpu.MemorySpace.HBM) if i in far else value
        for i, value in enumerate(args)
    ]
    return pl.pallas_call(
        kernel,
        out_shape=[jax.ShapeDtypeStruct(shape, dtype) for shape, dtype in outs],
        in_specs=[
            pl.BlockSpec(memory_space=pl.ANY if i in far or i in unread else VMEM)
            for i in range(len(args))
        ],
        out_specs=[
            pl.BlockSpec(memory_space=pl.ANY if i in far_out else VMEM) for i in range(len(outs))
        ],
        scratch_shapes=list(scratch),
        compiler_params=pltpu.CompilerParams(vmem_limit_bytes=limit << 20),
    )(*args)


def block_cols(step, core, cols):
    chip = (lax.axis_index("tp") // CORES) ^ step
    return pl.ds(pl.multiple_of((chip * CORES + core) * cols, cols), cols)


def split_kernel(depth, resid_ref, *refs):
    out_refs, sems = refs[:-1], refs[-1]
    copies = []
    for step, out_ref in enumerate(out_refs):
        start = pl.multiple_of((lax.axis_index("ep") ^ step) * depth, depth)
        copies.append(
            pltpu.make_async_copy(resid_ref.at[:, pl.ds(start, depth)], out_ref, sems.at[step])
        )
    for copy in copies:
        copy.start()
    for copy in copies:
        copy.wait()


def load_kernel(count, depth, gain_ref, *refs):
    sources, outs, sems = refs[:count], refs[count : 2 * count], refs[-1]
    start = pl.multiple_of(lax.axis_index("ep") * depth, depth)
    pairs = [(gain_ref.at[:, pl.ds(start, depth)], refs[2 * count])] + list(zip(sources, outs))
    copies = [
        pltpu.make_async_copy(source, target, sems.at[i])
        for i, (source, target) in enumerate(pairs)
    ]
    for copy in copies:
        copy.start()
    for copy in copies:
        copy.wait()


def gates_step(heads, cols, targets, outs, both_ref):
    igate_ref, fgate_ref, bias_ref, max_ref, rows_ref, row_ref = targets
    gates_ref, new_max_ref, factor_ref, own_ref = outs
    wide = rows_ref[...].astype(F32)
    factor = lax.rsqrt(jnp.mean(wide * wide, axis=1, keepdims=True) + EPSILON)
    normed = (wide * factor * row_ref[...]).astype(BF16)
    factor_ref[...] = jnp.broadcast_to(factor, factor_ref.shape)
    start = pl.multiple_of(lax.axis_index("tp") * cols, cols)
    own_ref[...] = rows_ref[:, pl.ds(start, cols)].astype(F32)
    all_heads = igate_ref.shape[0]
    square = (all_heads, all_heads)
    diagonal = lax.broadcasted_iota(jnp.int32, square, 0) == lax.broadcasted_iota(
        jnp.int32, square, 1
    )
    bias = jnp.sum(jnp.where(diagonal, bias_ref[...], 0.0), axis=1, keepdims=True)
    both_ref[:all_heads] = dot(igate_ref[...], normed, 1, 1)
    both_ref[all_heads:] = dot(fgate_ref[...], normed, 1, 1) + bias
    start = lax.axis_index("tp") * heads
    in_gate = both_ref[pl.ds(start, heads)]
    forget = both_ref[pl.ds(all_heads + start, heads)]
    log_forget = jnp.minimum(forget, 0.0) - jnp.log1p(jnp.exp(-jnp.abs(forget)))
    running = log_forget + max_ref[...]
    new_max = jnp.maximum(running, in_gate)
    new_max_ref[...] = new_max
    gates_ref[:heads] = jnp.exp(running - new_max)
    gates_ref[heads:] = jnp.exp(in_gate - new_max)


def slots_step(experts, local, ids_ref, picks_ref, at_ref):
    core = lax.axis_index("tp") % CORES
    topk, rows = ids_ref.shape
    slots = picks_ref.shape[0]
    capacity = slots // (experts // local)
    expert_iota = lax.broadcasted_iota(jnp.int32, (experts, rows), 0)
    hots = [(expert_iota == ids_ref[j : j + 1, :]).astype(F32) for j in range(topk)]
    before = lax.broadcasted_iota(jnp.int32, (rows, rows), 0) < lax.broadcasted_iota(
        jnp.int32, (rows, rows), 1
    )
    total = functools.reduce(lambda x, y: x + y, hots)
    earlier = dot(total.astype(BF16), before.astype(F32).astype(BF16), 1, 0)
    slot_iota = lax.broadcasted_iota(jnp.int32, (slots, rows), 0)
    picked = jnp.zeros((slots, rows), F32)
    for j in range(topk):
        ids = ids_ref[j : j + 1, :]
        slot = jnp.sum(earlier * hots[j], axis=0, keepdims=True).astype(jnp.int32)
        place = lax.shift_right_logical(ids, local.bit_length() - 1) ^ lax.axis_index("ep")
        at = jnp.where((ids & (local - 1)) == core, place * capacity + slot, -1)
        at_ref[j : j + 1, :] = at
        picked = picked + (slot_iota == at).astype(F32)
    picks_ref[...] = picked.astype(BF16)


def stage_kernel(skip, heads, chips, cols, experts, *refs):
    ids_ref, refs = refs[skip], refs[skip + 1 :]
    gate_sources, (w_ref, matrix_ref, normer_ref), pair = refs[:6], refs[6:9], refs[9:12]
    outs, scratch = refs[12:28], refs[28:]
    targets, both_ref, sems = scratch[:6], scratch[6], scratch[7]
    core = lax.axis_index("tp") % CORES
    away_ref, keep_ref, matrix_out, normer_out = outs[:4]
    pairs = list(zip(gate_sources, targets))
    for out_ref, target in ((away_ref, 1 - core), (keep_ref, core)):
        for k in range(chips):
            at = pl.ds(k * cols, cols)
            pairs.append((w_ref.at[:, block_cols(k, target, cols)], out_ref.at[:, at]))
    for i, source in enumerate(pair):
        pairs.append((source.at[1 - core], outs[4 + i]))
        pairs.append((source.at[core], outs[7 + i]))
    pairs += [(normer_ref, normer_out), (matrix_ref, matrix_out)]
    copies = [
        pltpu.make_async_copy(source, target, sems.at[i])
        for i, (source, target) in enumerate(pairs)
    ]
    for copy in copies:
        copy.start()
    slots_step(experts, pair[0].shape[0], ids_ref, outs[14], outs[15])
    for copy in copies[:6]:
        copy.wait()
    gates_step(heads, cols, targets, outs[10:14], both_ref)
    for copy in copies[6:]:
        copy.wait()


def update_kernel(heads, size, after_ref, matrix_ref, key_ref, value_ref, gates_ref, *refs):
    out_ref, done_ref, slots_ref, sems = refs
    copies = []
    for h in range(heads):
        slot = h % 2
        if h >= 2:
            copies[h - 2].wait()
        carried = gates_ref[h : h + 1, :]
        keys = key_ref[h] * gates_ref[heads + h : heads + h + 1, :]
        values = value_ref[h]
        for d in range(size):
            slots_ref[slot, d] = carried * matrix_ref[h, d] + keys[d : d + 1, :] * values
        copies.append(pltpu.make_async_copy(slots_ref.at[slot], out_ref.at[h], sems.at[slot]))
        copies[h].start()
    for copy in copies[-2:]:
        copy.wait()
    done_ref[...] = jnp.zeros_like(done_ref)


def project_kernel(x_ref, gain_ref, *refs):
    weights, out_ref = refs[:-1], refs[-1]
    cols = weights[0].shape[1]
    x = (x_ref[...].astype(F32) * gain_ref[...]).astype(BF16)
    for i, w_ref in enumerate(weights):
        out_ref[:, i * cols : (i + 1) * cols] = jnp.dot(
            x, w_ref[...], preferred_element_type=F32
        ).astype(out_ref.dtype)


def cell_kernel(heads, size, received, *refs):
    own_ref = refs[0]
    got_refs = refs[1 : 1 + received]
    gates_ref, matrix_ref, normer_ref, gain_ref, factor_ref = refs[1 + received : 6 + received]
    head_ref, key_ref, value_ref, norm_ref, turned_ref = refs[-5:]
    total = own_ref[...]
    for ref in got_refs:
        total = total + ref[...].astype(F32)
    total = total * factor_ref[:, :1]
    turned_ref[...] = total.astype(BF16).T.astype(F32)
    span = heads * size
    outs = []
    for h in range(heads):
        carried = gates_ref[h : h + 1, :]
        fresh = gates_ref[heads + h : heads + h + 1, :]
        scaled = turned_ref[h * size : (h + 1) * size, :] * size ** (-0.5)
        keys = turned_ref[span + h * size : span + (h + 1) * size, :]
        values = turned_ref[2 * span + h * size : 2 * span + (h + 1) * size, :]
        outgate = turned_ref[3 * span + h * size : 3 * span + (h + 1) * size, :]
        normer = normer_ref[h]
        readout = scaled[0:1, :] * matrix_ref[h, 0]
        for d in range(1, size):
            readout = readout + scaled[d : d + 1, :] * matrix_ref[h, d]
        score = jnp.sum(scaled * keys, axis=0, keepdims=True) * fresh
        numer = carried * readout + score * values
        denom = carried * jnp.sum(scaled * normer, axis=0, keepdims=True) + score
        cell = numer / jnp.maximum(jnp.abs(denom), 1.0)
        cell = cell * lax.rsqrt(jnp.mean(cell * cell, axis=0, keepdims=True) + EPSILON)
        outs.append(cell * jax.nn.sigmoid(outgate))
        key_ref[h] = keys
        value_ref[h] = values
        norm_ref[h] = carried * normer + fresh * keys
    head_ref[...] = (jnp.concatenate(outs, axis=0).T * gain_ref[...]).astype(BF16)


def mix_kernel(cols, own_ref, got_ref, w_own_ref, w_got_ref, keep_ref, *out_refs):
    own, got = own_ref[...], got_ref[...]
    for k, out_ref in enumerate((keep_ref,) + out_refs):
        at = slice(k * cols, (k + 1) * cols)
        value = jnp.dot(own, w_own_ref[:, at], preferred_element_type=F32)
        value = value + jnp.dot(got, w_got_ref[:, at], preferred_element_type=F32)
        out_ref[...] = value.astype(out_ref.dtype)


def final_kernel(*refs):
    total = refs[0][...].astype(F32)
    for ref in refs[1:-1]:
        total = total + ref[...].astype(F32)
    refs[-1][...] = total.astype(BF16)


def after_kernel(done_ref, *refs):
    final_kernel(*refs)


def route_kernel(per_group, normed_ref, group_ref, expert_ref, ids_ref, at_ref, *refs):
    high_ref, low_ref = refs
    rows, slots = high_ref.shape
    groups, experts = group_ref.shape[0], expert_ref.shape[0]
    group_exp = jnp.exp(dot(group_ref[...], normed_ref[...], 1, 1))
    group_prob = group_exp / jnp.sum(group_exp, axis=0, keepdims=True)
    logits = dot(expert_ref[...], normed_ref[...], 1, 1)
    expert_iota = lax.broadcasted_iota(jnp.int32, (experts, rows), 0)
    group_iota = lax.broadcasted_iota(jnp.int32, (groups, rows), 0)
    slot_iota = lax.broadcasted_iota(jnp.int32, (slots, rows), 0)
    chosen, shares = [], []
    for j in range(ids_ref.shape[0]):
        ids = ids_ref[j : j + 1, :]
        hot = expert_iota == ids
        chosen.append(jnp.exp(jnp.sum(jnp.where(hot, logits, 0.0), axis=0, keepdims=True)))
        first = group_iota * per_group
        hot = (first <= ids) & (ids < first + per_group)
        shares.append(jnp.sum(jnp.where(hot, group_prob, 0.0), axis=0, keepdims=True))
    total = functools.reduce(lambda x, y: x + y, chosen)
    combine = jnp.zeros((slots, rows), F32)
    for j, (value, share) in enumerate(zip(chosen, shares)):
        weight = share * (value / total)
        combine = combine + jnp.where(slot_iota == at_ref[j : j + 1, :], weight, 0.0)
    combine = combine.T
    high = combine.astype(BF16)
    high_ref[...] = high
    low_ref[...] = (combine - high.astype(F32)).astype(BF16)


def dispatch_kernel(chips, cols, capacity, *refs):
    own_refs = refs[:chips]
    other_refs, refs = refs[chips : 2 * chips], refs[2 * chips :]
    gain_ref, pick_ref, normed_ref = refs[:3]
    out_refs, full_ref = refs[3:-1], refs[-1]
    core = lax.axis_index("tp") % CORES
    for k in range(chips):
        full_ref[:, block_cols(k, core, cols)] = own_refs[k][...].astype(F32)
        full_ref[:, block_cols(k, 1 - core, cols)] = other_refs[k][...].astype(F32)
    full = full_ref[...]
    factor = lax.rsqrt(jnp.sum(full * full, axis=1, keepdims=True) / full.shape[1] + EPSILON)
    normed = (full * factor * gain_ref[...]).astype(BF16)
    normed_ref[...] = normed
    picked = jnp.dot(pick_ref[...], normed, preferred_element_type=F32)
    for k, out_ref in enumerate(out_refs):
        out_ref[...] = picked[k * capacity : (k + 1) * capacity].astype(BF16)


def expert_kernel(x_ref, *refs):
    weights, out_ref = refs[:6], refs[6]
    x = x_ref[...]
    result = None
    for gate_ref, up_ref, down_ref in (weights[:3], weights[3:]):
        gate = jnp.dot(x, gate_ref[...], preferred_element_type=F32)
        up = jnp.dot(x, up_ref[...], preferred_element_type=F32)
        units = (jax.nn.silu(gate) * up).astype(BF16)
        part = jnp.dot(units, down_ref[...], preferred_element_type=F32)
        result = part if result is None else result + part
    out_ref[...] = result.astype(BF16)


def combine_kernel(chips, cols, blocks, *refs):
    y_refs = refs[:blocks]
    high_ref, low_ref = refs[blocks : blocks + 2]
    away_refs, keep_refs = refs[blocks + 2 : blocks + 2 + chips], refs[blocks + 2 + chips :]
    core = lax.axis_index("tp") % CORES
    for k in range(chips):
        for target, out_ref in ((1 - core, away_refs[k]), (core, keep_refs[k])):
            ds = block_cols(k, target, cols)
            y = jnp.concatenate([ref[:, ds] for ref in y_refs], axis=0)
            value = jnp.dot(high_ref[...], y, preferred_element_type=F32)
            value = value + jnp.dot(low_ref[...], y, preferred_element_type=F32)
            out_ref[...] = value.astype(out_ref.dtype)


def per_device(
    resid,
    norm1_gain,
    w_query,
    w_key,
    w_value,
    w_outgate,
    w_igate,
    w_fgate,
    forget_bias,
    head_gain,
    w_out,
    state_matrix,
    state_norm,
    state_max,
    norm2_gain,
    group_router,
    expert_router,
    expert_ids,
    exp_gate,
    exp_up,
    exp_down,
):
    rows, width = resid.shape
    heads, size = state_matrix.shape[1], state_matrix.shape[2]
    ep_count, tp_count = lax.axis_size("ep"), lax.axis_size("tp")
    chips = tp_count // CORES
    cols = width // tp_count
    depth = w_query.shape[0]
    experts_all, groups = expert_router.shape[1], group_router.shape[1]
    per_group = experts_all // groups
    topk = expert_ids.shape[1]
    local_experts, _, _ = exp_gate.shape
    assert local_experts == CORES
    capacity = max(2, 3 * rows * topk // (2 * experts_all))
    half = chips * cols
    others = range(1, ep_count)

    blocks = call(
        functools.partial(split_kernel, depth),
        [((rows, depth), BF16)] * ep_count,
        resid,
        far=(0,),
        scratch=[pltpu.SemaphoreType.DMA((ep_count,))],
    )
    arrived = [ep_send(blocks[k], k) for k in others]
    matrix = state_matrix.transpose(1, 2, 3, 0)
    normer = state_norm.transpose(1, 2, 0)
    weights = (w_query, w_key, w_value, w_outgate)
    *weights, gain = call(
        functools.partial(load_kernel, len(weights), depth),
        [(value.shape, value.dtype) for value in weights] + [((1, depth), F32)],
        norm1_gain[None, :],
        *weights,
        far=range(1 + len(weights)),
        scratch=[pltpu.SemaphoreType.DMA((1 + len(weights),))],
    )
    weights = [gain] + weights
    span = 4 * heads * size
    (own,) = call(project_kernel, [((rows, span), F32)], blocks[0], *weights)
    parts, sent = [], []
    for k in others:
        (part,) = call(project_kernel, [((rows, span), BF16)], arrived[k - 1], *weights)
        parts.append(part)
        sent.append(ep_send(part, k))

    all_heads = w_igate.shape[1]
    slots = ep_count * capacity
    pair = (exp_gate, exp_up, exp_down)
    expert_outs = [(value.shape[1:], value.dtype) for value in pair]
    w_sent, w_own, matrix, normer, *staged = call(
        functools.partial(stage_kernel, len(parts), heads, chips, cols, experts_all),
        [((heads * size, half), BF16)] * 2
        + [(matrix.shape, F32), (normer.shape, F32)]
        + expert_outs * 2
        + [((2 * heads, rows), F32), ((heads, rows), F32)]
        + [((rows, 128), F32), ((rows, cols), F32)]
        + [((slots, rows), BF16), ((topk, rows), jnp.int32)],
        *parts,
        expert_ids.T,
        w_igate.T,
        w_fgate.T,
        forget_bias[None, :],
        state_max.T,
        resid,
        norm1_gain[None, :],
        w_out,
        matrix,
        normer,
        *pair,
        far=range(len(parts) + 1, len(parts) + 13),
        unread=range(len(parts)),
        scratch=[
            pltpu.VMEM((all_heads, width), BF16),
            pltpu.VMEM((all_heads, width), BF16),
            pltpu.VMEM((1, all_heads), F32),
            pltpu.VMEM((heads, rows), F32),
            pltpu.VMEM((rows, width), BF16),
            pltpu.VMEM((1, width), F32),
            pltpu.VMEM((2 * all_heads, rows), F32),
            pltpu.SemaphoreType.DMA((14 + 2 * chips,)),
        ],
        limit=24,
    )
    expert_sent, expert_mine = staged[:3], staged[3:6]
    gates, new_max, factor, own_resid, picks, places = staged[6:]
    w_got = core_send(w_sent)
    expert_got = [core_send(value) for value in expert_sent]

    head_out, key_rows, value_rows, new_normer = call(
        functools.partial(cell_kernel, heads, size, ep_count - 1),
        [((rows, heads * size), BF16)] + [((heads, size, rows), F32)] * 3,
        own,
        *sent,
        gates,
        matrix,
        normer,
        head_gain[None, :],
        factor,
        w_got,
        unread=(ep_count + 5,),
        scratch=[pltpu.VMEM((span, rows), F32)],
        limit=20,
    )

    mix_own, *mix_sent = call(
        functools.partial(mix_kernel, cols),
        [((rows, cols), F32)] + [((rows, cols), BF16)] * (chips - 1),
        head_out,
        core_send(head_out),
        w_own,
        w_got,
    )
    mix_got = [chip_send(mix_sent[k - 1], k) for k in range(1, chips)]

    new_matrix, done = call(
        functools.partial(update_kernel, heads, size),
        [((heads, size, size, rows), F32), ((8, 128), F32)],
        mix_sent[-1],
        matrix,
        key_rows,
        value_rows,
        gates,
        unread=(0,),
        far_out=(0,),
        scratch=[pltpu.VMEM((2, size, size, rows), F32), pltpu.SemaphoreType.DMA((2,))],
        limit=14,
    )

    (after_cols,) = call(
        after_kernel,
        [((rows, cols), BF16)],
        done,
        own_resid,
        mix_own,
        *mix_got,
        unread=(0,),
        limit=4,
    )
    after_parts = [after_cols] + [chip_send(after_cols, k) for k in range(1, chips)]
    after_others = [core_send(part) for part in after_parts]

    normed2, *buffers = call(
        functools.partial(dispatch_kernel, chips, cols, capacity),
        [((rows, width), BF16)] + [((capacity, width), BF16)] * ep_count,
        *after_parts,
        *after_others,
        norm2_gain[None, :],
        picks,
        scratch=[pltpu.VMEM((rows, width), F32)],
        limit=10,
    )
    taken = [buffers[0]] + [ep_send(buffers[k], k) for k in others]

    combine_high, combine_low = call(
        functools.partial(route_kernel, per_group),
        [((rows, slots), BF16)] * 2,
        normed2,
        group_router.T,
        expert_router.T,
        expert_ids.T,
        places,
    )

    terms = []
    for k in range(ep_count):
        (part,) = call(
            expert_kernel,
            [((capacity, width), BF16)],
            taken[k],
            *expert_mine,
            *expert_got,
            limit=12,
        )
        terms.append(part)
    back = [terms[0]] + [ep_send(terms[k], k) for k in others]
    moe_blocks = call(
        functools.partial(combine_kernel, chips, cols, ep_count),
        [((rows, cols), BF16)] * chips + [((rows, cols), F32)] * chips,
        *back,
        combine_high,
        combine_low,
    )
    moe_parts = [moe_blocks[chips + k] + core_send(moe_blocks[k]).astype(F32) for k in range(chips)]
    moe_got = [chip_send(moe_parts[k].astype(BF16), k) for k in range(1, chips)]
    (mixed,) = call(
        final_kernel, [((rows, cols), BF16)], after_cols, moe_parts[0], *moe_got, limit=4
    )
    return (
        mixed,
        new_matrix.transpose(3, 0, 1, 2),
        new_normer.transpose(2, 0, 1),
        new_max.T,
    )


def solution(mesh):
    in_specs = (
        P("ep", None),
        P(),
        P("ep", "tp"),
        P("ep", "tp"),
        P("ep", "tp"),
        P("ep", "tp"),
        P(),
        P(),
        P(),
        P("tp"),
        P("tp", None),
        P("ep", "tp", None, None),
        P("ep", "tp", None),
        P("ep", "tp"),
        P(),
        P(),
        P(),
        P("ep", None),
        P("ep", None, "tp"),
        P("ep", None, "tp"),
        P("ep", "tp", None),
    )
    out_specs = (P("ep", "tp"), P("ep", "tp", None, None), P("ep", "tp", None), P("ep", "tp"))
    return jax.shard_map(
        per_device, mesh=mesh, in_specs=in_specs, out_specs=out_specs, check_vma=False
    )
```

```python
import functools

import jax
import jax.numpy as jnp
from jax import lax
from jax.experimental import pallas as pl
from jax.experimental.pallas import tpu as pltpu
from jax.sharding import PartitionSpec as P


EPSILON = 1e-06
CORES = 2
VMEM = pltpu.MemorySpace.VMEM
F32, BF16 = jnp.float32, jnp.bfloat16


def ep_send(value, step):
    count = lax.axis_size("ep")
    return lax.ppermute(value, "ep", [(i, i ^ step) for i in range(count)])


def chip_send(value, step):
    count = lax.axis_size("tp")
    return lax.ppermute(value, "tp", [(i, i ^ (CORES * step)) for i in range(count)])


def core_send(value):
    count = lax.axis_size("tp")
    return lax.ppermute(value, "tp", [(i, i ^ 1) for i in range(count)])


def dot(lhs, rhs, lhs_dim, rhs_dim):
    return lax.dot_general(
        lhs, rhs, (((lhs_dim,), (rhs_dim,)), ((), ())), preferred_element_type=F32
    )


def call(kernel, outs, *args, far=(), unread=(), far_out=(), scratch=(), limit=8):
    args = [
        pltpu.with_memory_space_constraint(value, pltpu.MemorySpace.HBM) if i in far else value
        for i, value in enumerate(args)
    ]
    return pl.pallas_call(
        kernel,
        out_shape=[jax.ShapeDtypeStruct(shape, dtype) for shape, dtype in outs],
        in_specs=[
            pl.BlockSpec(memory_space=pl.ANY if i in far or i in unread else VMEM)
            for i in range(len(args))
        ],
        out_specs=[
            pl.BlockSpec(memory_space=pl.ANY if i in far_out else VMEM) for i in range(len(outs))
        ],
        scratch_shapes=list(scratch),
        compiler_params=pltpu.CompilerParams(vmem_limit_bytes=limit << 20),
    )(*args)


def block_cols(step, core, cols):
    chip = (lax.axis_index("tp") // CORES) ^ step
    return pl.ds(pl.multiple_of((chip * CORES + core) * cols, cols), cols)


def split_kernel(depth, resid_ref, *refs):
    out_refs, sems = refs[:-1], refs[-1]
    copies = []
    for step, out_ref in enumerate(out_refs):
        start = pl.multiple_of((lax.axis_index("ep") ^ step) * depth, depth)
        copies.append(
            pltpu.make_async_copy(resid_ref.at[:, pl.ds(start, depth)], out_ref, sems.at[step])
        )
    for copy in copies:
        copy.start()
    for copy in copies:
        copy.wait()


def load_kernel(count, depth, gain_ref, *refs):
    sources, outs, sems = refs[:count], refs[count : 2 * count], refs[-1]
    start = pl.multiple_of(lax.axis_index("ep") * depth, depth)
    pairs = [(gain_ref.at[:, pl.ds(start, depth)], refs[2 * count])] + list(zip(sources, outs))
    copies = [
        pltpu.make_async_copy(source, target, sems.at[i])
        for i, (source, target) in enumerate(pairs)
    ]
    for copy in copies:
        copy.start()
    for copy in copies:
        copy.wait()


def gates_step(heads, cols, targets, outs, both_ref):
    igate_ref, fgate_ref, bias_ref, max_ref, rows_ref, row_ref = targets
    gates_ref, new_max_ref, factor_ref, own_ref = outs
    wide = rows_ref[...].astype(F32)
    factor = lax.rsqrt(jnp.mean(wide * wide, axis=1, keepdims=True) + EPSILON)
    normed = (wide * factor * row_ref[...]).astype(BF16)
    factor_ref[...] = jnp.broadcast_to(factor, factor_ref.shape)
    start = pl.multiple_of(lax.axis_index("tp") * cols, cols)
    own_ref[...] = rows_ref[:, pl.ds(start, cols)].astype(F32)
    all_heads = igate_ref.shape[0]
    square = (all_heads, all_heads)
    diagonal = lax.broadcasted_iota(jnp.int32, square, 0) == lax.broadcasted_iota(
        jnp.int32, square, 1
    )
    bias = jnp.sum(jnp.where(diagonal, bias_ref[...], 0.0), axis=1, keepdims=True)
    both_ref[:all_heads] = dot(igate_ref[...], normed, 1, 1)
    both_ref[all_heads:] = dot(fgate_ref[...], normed, 1, 1) + bias
    start = lax.axis_index("tp") * heads
    in_gate = both_ref[pl.ds(start, heads)]
    forget = both_ref[pl.ds(all_heads + start, heads)]
    log_forget = jnp.minimum(forget, 0.0) - jnp.log1p(jnp.exp(-jnp.abs(forget)))
    running = log_forget + max_ref[...]
    new_max = jnp.maximum(running, in_gate)
    new_max_ref[...] = new_max
    gates_ref[:heads] = jnp.exp(running - new_max)
    gates_ref[heads:] = jnp.exp(in_gate - new_max)


def slots_step(experts, local, ids_ref, picks_ref, at_ref):
    core = lax.axis_index("tp") % CORES
    topk, rows = ids_ref.shape
    slots = picks_ref.shape[0]
    capacity = slots // (experts // local)
    expert_iota = lax.broadcasted_iota(jnp.int32, (experts, rows), 0)
    hots = [(expert_iota == ids_ref[j : j + 1, :]).astype(F32) for j in range(topk)]
    before = lax.broadcasted_iota(jnp.int32, (rows, rows), 0) < lax.broadcasted_iota(
        jnp.int32, (rows, rows), 1
    )
    total = functools.reduce(lambda x, y: x + y, hots)
    earlier = dot(total.astype(BF16), before.astype(F32).astype(BF16), 1, 0)
    slot_iota = lax.broadcasted_iota(jnp.int32, (slots, rows), 0)
    picked = jnp.zeros((slots, rows), F32)
    for j in range(topk):
        ids = ids_ref[j : j + 1, :]
        slot = jnp.sum(earlier * hots[j], axis=0, keepdims=True).astype(jnp.int32)
        place = lax.shift_right_logical(ids, local.bit_length() - 1) ^ lax.axis_index("ep")
        at = jnp.where((ids & (local - 1)) == core, place * capacity + slot, -1)
        at_ref[j : j + 1, :] = at
        picked = picked + (slot_iota == at).astype(F32)
    picks_ref[...] = picked.astype(BF16)


def stage_kernel(skip, heads, chips, cols, experts, *refs):
    ids_ref, refs = refs[skip], refs[skip + 1 :]
    gate_sources, (w_ref, matrix_ref, normer_ref), pair = refs[:6], refs[6:9], refs[9:12]
    outs, scratch = refs[12:28], refs[28:]
    targets, both_ref, sems = scratch[:6], scratch[6], scratch[7]
    core = lax.axis_index("tp") % CORES
    away_ref, keep_ref, matrix_out, normer_out = outs[:4]
    pairs = list(zip(gate_sources, targets))
    for out_ref, target in ((away_ref, 1 - core), (keep_ref, core)):
        for k in range(chips):
            at = pl.ds(k * cols, cols)
            pairs.append((w_ref.at[:, block_cols(k, target, cols)], out_ref.at[:, at]))
    for i, source in enumerate(pair):
        pairs.append((source.at[1 - core], outs[4 + i]))
        pairs.append((source.at[core], outs[7 + i]))
    pairs += [(normer_ref, normer_out), (matrix_ref, matrix_out)]
    copies = [
        pltpu.make_async_copy(source, target, sems.at[i])
        for i, (source, target) in enumerate(pairs)
    ]
    for copy in copies:
        copy.start()
    slots_step(experts, pair[0].shape[0], ids_ref, outs[14], outs[15])
    for copy in copies[:6]:
        copy.wait()
    gates_step(heads, cols, targets, outs[10:14], both_ref)
    for copy in copies[6:]:
        copy.wait()


def update_kernel(heads, size, after_ref, matrix_ref, key_ref, value_ref, gates_ref, *refs):
    out_ref, done_ref, slots_ref, sems = refs
    copies = []
    for h in range(heads):
        slot = h % 2
        if h >= 2:
            copies[h - 2].wait()
        carried = gates_ref[h : h + 1, :]
        keys = key_ref[h] * gates_ref[heads + h : heads + h + 1, :]
        values = value_ref[h]
        for d in range(size):
            slots_ref[slot, d] = carried * matrix_ref[h, d] + keys[d : d + 1, :] * values
        copies.append(pltpu.make_async_copy(slots_ref.at[slot], out_ref.at[h], sems.at[slot]))
        copies[h].start()
    for copy in copies[-2:]:
        copy.wait()
    done_ref[...] = jnp.zeros_like(done_ref)


def project_kernel(x_ref, gain_ref, *refs):
    weights, out_ref = refs[:-1], refs[-1]
    cols = weights[0].shape[1]
    x = (x_ref[...].astype(F32) * gain_ref[...]).astype(BF16)
    for i, w_ref in enumerate(weights):
        out_ref[:, i * cols : (i + 1) * cols] = jnp.dot(
            x, w_ref[...], preferred_element_type=F32
        ).astype(out_ref.dtype)


def sum_kernel(*refs):
    total = refs[0][...]
    for ref in refs[1:-1]:
        total = total + ref[...].astype(F32)
    refs[-1][...] = total


def cell_kernel(heads, size, received, *refs):
    own_ref = refs[0]
    got_refs = refs[1 : 1 + received]
    gates_ref, matrix_ref, normer_ref, gain_ref, factor_ref = refs[1 + received : 6 + received]
    head_ref, key_ref, value_ref, norm_ref, turned_ref = refs[-5:]
    total = own_ref[...]
    for ref in got_refs:
        total = total + ref[...].astype(F32)
    total = total * factor_ref[:, :1]
    turned_ref[...] = total.astype(BF16).T.astype(F32)
    span = heads * size
    outs = []
    for h in range(heads):
        carried = gates_ref[h : h + 1, :]
        fresh = gates_ref[heads + h : heads + h + 1, :]
        scaled = turned_ref[h * size : (h + 1) * size, :] * size ** (-0.5)
        keys = turned_ref[span + h * size : span + (h + 1) * size, :]
        values = turned_ref[2 * span + h * size : 2 * span + (h + 1) * size, :]
        outgate = turned_ref[3 * span + h * size : 3 * span + (h + 1) * size, :]
        normer = normer_ref[h]
        readout = scaled[0:1, :] * matrix_ref[h, 0]
        for d in range(1, size):
            readout = readout + scaled[d : d + 1, :] * matrix_ref[h, d]
        score = jnp.sum(scaled * keys, axis=0, keepdims=True) * fresh
        numer = carried * readout + score * values
        denom = carried * jnp.sum(scaled * normer, axis=0, keepdims=True) + score
        cell = numer / jnp.maximum(jnp.abs(denom), 1.0)
        cell = cell * lax.rsqrt(jnp.mean(cell * cell, axis=0, keepdims=True) + EPSILON)
        outs.append(cell * jax.nn.sigmoid(outgate))
        key_ref[h] = keys
        value_ref[h] = values
        norm_ref[h] = carried * normer + fresh * keys
    head_ref[...] = (jnp.concatenate(outs, axis=0).T * gain_ref[...]).astype(BF16)


def mix_kernel(cols, own_ref, got_ref, w_own_ref, w_got_ref, keep_ref, *out_refs):
    own, got = own_ref[...], got_ref[...]
    for k, out_ref in enumerate((keep_ref,) + out_refs):
        at = slice(k * cols, (k + 1) * cols)
        value = jnp.dot(own, w_own_ref[:, at], preferred_element_type=F32)
        value = value + jnp.dot(got, w_got_ref[:, at], preferred_element_type=F32)
        out_ref[...] = value.astype(out_ref.dtype)


def final_kernel(*refs):
    total = refs[0][...].astype(F32)
    for ref in refs[1:-1]:
        total = total + ref[...].astype(F32)
    refs[-1][...] = total.astype(BF16)


def after_kernel(done_ref, *refs):
    final_kernel(*refs)


def route_kernel(per_group, normed_ref, group_ref, expert_ref, ids_ref, at_ref, *refs):
    high_ref, low_ref = refs
    rows, slots = high_ref.shape
    groups, experts = group_ref.shape[0], expert_ref.shape[0]
    group_exp = jnp.exp(dot(group_ref[...], normed_ref[...], 1, 1))
    group_prob = group_exp / jnp.sum(group_exp, axis=0, keepdims=True)
    logits = dot(expert_ref[...], normed_ref[...], 1, 1)
    expert_iota = lax.broadcasted_iota(jnp.int32, (experts, rows), 0)
    group_iota = lax.broadcasted_iota(jnp.int32, (groups, rows), 0)
    slot_iota = lax.broadcasted_iota(jnp.int32, (slots, rows), 0)
    chosen, shares = [], []
    for j in range(ids_ref.shape[0]):
        ids = ids_ref[j : j + 1, :]
        hot = expert_iota == ids
        chosen.append(jnp.exp(jnp.sum(jnp.where(hot, logits, 0.0), axis=0, keepdims=True)))
        first = group_iota * per_group
        hot = (first <= ids) & (ids < first + per_group)
        shares.append(jnp.sum(jnp.where(hot, group_prob, 0.0), axis=0, keepdims=True))
    total = functools.reduce(lambda x, y: x + y, chosen)
    combine = jnp.zeros((slots, rows), F32)
    for j, (value, share) in enumerate(zip(chosen, shares)):
        weight = share * (value / total)
        combine = combine + jnp.where(slot_iota == at_ref[j : j + 1, :], weight, 0.0)
    combine = combine.T
    high = combine.astype(BF16)
    high_ref[...] = high
    low_ref[...] = (combine - high.astype(F32)).astype(BF16)


def dispatch_kernel(chips, cols, capacity, *refs):
    own_refs = refs[:chips]
    other_refs, refs = refs[chips : 2 * chips], refs[2 * chips :]
    gain_ref, pick_ref, normed_ref = refs[:3]
    out_refs, full_ref = refs[3:-1], refs[-1]
    core = lax.axis_index("tp") % CORES
    for k in range(chips):
        full_ref[:, block_cols(k, core, cols)] = own_refs[k][...].astype(F32)
        full_ref[:, block_cols(k, 1 - core, cols)] = other_refs[k][...].astype(F32)
    full = full_ref[...]
    factor = lax.rsqrt(jnp.sum(full * full, axis=1, keepdims=True) / full.shape[1] + EPSILON)
    normed = (full * factor * gain_ref[...]).astype(BF16)
    normed_ref[...] = normed
    picked = jnp.dot(pick_ref[...], normed, preferred_element_type=F32)
    for k, out_ref in enumerate(out_refs):
        out_ref[...] = picked[k * capacity : (k + 1) * capacity].astype(BF16)


def expert_kernel(x_ref, *refs):
    weights, out_ref = refs[:6], refs[6]
    x = x_ref[...]
    result = None
    for gate_ref, up_ref, down_ref in (weights[:3], weights[3:]):
        gate = jnp.dot(x, gate_ref[...], preferred_element_type=F32)
        up = jnp.dot(x, up_ref[...], preferred_element_type=F32)
        units = (jax.nn.silu(gate) * up).astype(BF16)
        part = jnp.dot(units, down_ref[...], preferred_element_type=F32)
        result = part if result is None else result + part
    out_ref[...] = result.astype(BF16)


def combine_kernel(chips, cols, blocks, *refs):
    y_refs = refs[:blocks]
    high_ref, low_ref = refs[blocks : blocks + 2]
    away_refs, keep_refs = refs[blocks + 2 : blocks + 2 + chips], refs[blocks + 2 + chips :]
    core = lax.axis_index("tp") % CORES
    for k in range(chips):
        for target, out_ref in ((1 - core, away_refs[k]), (core, keep_refs[k])):
            ds = block_cols(k, target, cols)
            y = jnp.concatenate([ref[:, ds] for ref in y_refs], axis=0)
            value = jnp.dot(high_ref[...], y, preferred_element_type=F32)
            value = value + jnp.dot(low_ref[...], y, preferred_element_type=F32)
            out_ref[...] = value.astype(out_ref.dtype)


def per_device(
    resid,
    norm1_gain,
    w_query,
    w_key,
    w_value,
    w_outgate,
    w_igate,
    w_fgate,
    forget_bias,
    head_gain,
    w_out,
    state_matrix,
    state_norm,
    state_max,
    norm2_gain,
    group_router,
    expert_router,
    expert_ids,
    exp_gate,
    exp_up,
    exp_down,
):
    rows, width = resid.shape
    heads, size = state_matrix.shape[1], state_matrix.shape[2]
    ep_count, tp_count = lax.axis_size("ep"), lax.axis_size("tp")
    chips = tp_count // CORES
    cols = width // tp_count
    depth = w_query.shape[0]
    experts_all, groups = expert_router.shape[1], group_router.shape[1]
    per_group = experts_all // groups
    topk = expert_ids.shape[1]
    local_experts, _, _ = exp_gate.shape
    assert local_experts == CORES
    capacity = max(2, 3 * rows * topk // (2 * experts_all))
    half = chips * cols
    others = range(1, ep_count)

    blocks = call(
        functools.partial(split_kernel, depth),
        [((rows, depth), BF16)] * ep_count,
        resid,
        far=(0,),
        scratch=[pltpu.SemaphoreType.DMA((ep_count,))],
    )
    arrived = [ep_send(blocks[k], k) for k in others]
    matrix = state_matrix.transpose(1, 2, 3, 0)
    normer = state_norm.transpose(1, 2, 0)
    weights = (w_query, w_key, w_value, w_outgate)
    *weights, gain = call(
        functools.partial(load_kernel, len(weights), depth),
        [(value.shape, value.dtype) for value in weights] + [((1, depth), F32)],
        norm1_gain[None, :],
        *weights,
        far=range(1 + len(weights)),
        scratch=[pltpu.SemaphoreType.DMA((1 + len(weights),))],
    )
    weights = [gain] + weights
    span = 4 * heads * size
    (own,) = call(project_kernel, [((rows, span), F32)], blocks[0], *weights)
    parts, sent = [], []
    for k in others:
        (part,) = call(project_kernel, [((rows, span), BF16)], arrived[k - 1], *weights)
        parts.append(part)
        sent.append(ep_send(part, k))

    all_heads = w_igate.shape[1]
    slots = ep_count * capacity
    pair = (exp_gate, exp_up, exp_down)
    expert_outs = [(value.shape[1:], value.dtype) for value in pair]
    w_sent, w_own, matrix, normer, *staged = call(
        functools.partial(stage_kernel, len(parts), heads, chips, cols, experts_all),
        [((heads * size, half), BF16)] * 2
        + [(matrix.shape, F32), (normer.shape, F32)]
        + expert_outs * 2
        + [((2 * heads, rows), F32), ((heads, rows), F32)]
        + [((rows, 128), F32), ((rows, cols), F32)]
        + [((slots, rows), BF16), ((topk, rows), jnp.int32)],
        *parts,
        expert_ids.T,
        w_igate.T,
        w_fgate.T,
        forget_bias[None, :],
        state_max.T,
        resid,
        norm1_gain[None, :],
        w_out,
        matrix,
        normer,
        *pair,
        far=range(len(parts) + 1, len(parts) + 13),
        unread=range(len(parts)),
        scratch=[
            pltpu.VMEM((all_heads, width), BF16),
            pltpu.VMEM((all_heads, width), BF16),
            pltpu.VMEM((1, all_heads), F32),
            pltpu.VMEM((heads, rows), F32),
            pltpu.VMEM((rows, width), BF16),
            pltpu.VMEM((1, width), F32),
            pltpu.VMEM((2 * all_heads, rows), F32),
            pltpu.SemaphoreType.DMA((14 + 2 * chips,)),
        ],
        limit=24,
    )
    expert_sent, expert_mine = staged[:3], staged[3:6]
    gates, new_max, factor, own_resid, picks, places = staged[6:]
    w_got = core_send(w_sent)
    expert_got = [core_send(value) for value in expert_sent]

    (early,) = call(sum_kernel, [((rows, span), F32)], own, *sent[1:])
    head_out, key_rows, value_rows, new_normer = call(
        functools.partial(cell_kernel, heads, size, 1),
        [((rows, heads * size), BF16)] + [((heads, size, rows), F32)] * 3,
        early,
        sent[0],
        gates,
        matrix,
        normer,
        head_gain[None, :],
        factor,
        w_got,
        unread=(7,),
        scratch=[pltpu.VMEM((span, rows), F32)],
        limit=20,
    )

    mix_own, *mix_sent = call(
        functools.partial(mix_kernel, cols),
        [((rows, cols), F32)] + [((rows, cols), BF16)] * (chips - 1),
        head_out,
        core_send(head_out),
        w_own,
        w_got,
    )
    mix_got = [chip_send(mix_sent[k - 1], k) for k in range(1, chips)]

    new_matrix, done = call(
        functools.partial(update_kernel, heads, size),
        [((heads, size, size, rows), F32), ((8, 128), F32)],
        mix_sent[-1],
        matrix,
        key_rows,
        value_rows,
        gates,
        unread=(0,),
        far_out=(0,),
        scratch=[pltpu.VMEM((2, size, size, rows), F32), pltpu.SemaphoreType.DMA((2,))],
        limit=14,
    )

    (after_cols,) = call(
        after_kernel,
        [((rows, cols), BF16)],
        done,
        own_resid,
        mix_own,
        *mix_got,
        unread=(0,),
        limit=4,
    )
    after_parts = [after_cols] + [chip_send(after_cols, k) for k in range(1, chips)]
    after_others = [core_send(part) for part in after_parts]

    normed2, *buffers = call(
        functools.partial(dispatch_kernel, chips, cols, capacity),
        [((rows, width), BF16)] + [((capacity, width), BF16)] * ep_count,
        *after_parts,
        *after_others,
        norm2_gain[None, :],
        picks,
        scratch=[pltpu.VMEM((rows, width), F32)],
        limit=10,
    )
    taken = [buffers[0]] + [ep_send(buffers[k], k) for k in others]

    combine_high, combine_low = call(
        functools.partial(route_kernel, per_group),
        [((rows, slots), BF16)] * 2,
        normed2,
        group_router.T,
        expert_router.T,
        expert_ids.T,
        places,
    )

    terms = []
    for k in range(ep_count):
        (part,) = call(
            expert_kernel,
            [((capacity, width), BF16)],
            taken[k],
            *expert_mine,
            *expert_got,
            limit=12,
        )
        terms.append(part)
    back = [terms[0]] + [ep_send(terms[k], k) for k in others]
    moe_blocks = call(
        functools.partial(combine_kernel, chips, cols, ep_count),
        [((rows, cols), BF16)] * chips + [((rows, cols), F32)] * chips,
        *back,
        combine_high,
        combine_low,
    )
    moe_parts = [moe_blocks[chips + k] + core_send(moe_blocks[k]).astype(F32) for k in range(chips)]
    moe_got = [chip_send(moe_parts[k].astype(BF16), k) for k in range(1, chips)]
    (mixed,) = call(
        final_kernel, [((rows, cols), BF16)], after_cols, moe_parts[0], *moe_got, limit=4
    )
    return (
        mixed,
        new_matrix.transpose(3, 0, 1, 2),
        new_normer.transpose(2, 0, 1),
        new_max.T,
    )


def solution(mesh):
    in_specs = (
        P("ep", None),
        P(),
        P("ep", "tp"),
        P("ep", "tp"),
        P("ep", "tp"),
        P("ep", "tp"),
        P(),
        P(),
        P(),
        P("tp"),
        P("tp", None),
        P("ep", "tp", None, None),
        P("ep", "tp", None),
        P("ep", "tp"),
        P(),
        P(),
        P(),
        P("ep", None),
        P("ep", None, "tp"),
        P("ep", None, "tp"),
        P("ep", "tp", None),
    )
    out_specs = (P("ep", "tp"), P("ep", "tp", None, None), P("ep", "tp", None), P("ep", "tp"))
    return jax.shard_map(
        per_device, mesh=mesh, in_specs=in_specs, out_specs=out_specs, check_vma=False
    )
```
